32 devices in a mesh: kv: 8 (over z, y), tp: 4 (over x, core).
Axes of the slice: x: 2, y: 2, z: 4, core: 2. Of those that a mesh axis runs over, the one named last changes fastest.
Arguments:
- tokens: bfloat16 [16, 4096], P(None, ('kv', 'tp')), may hold values from -8 to 8
- gate_weights: bfloat16 [2, 4096, 11264], P(None, None, ('kv', 'tp')), may hold values from -0.09375 to 0.09375
- up_weights: bfloat16 [2, 4096, 11264], P(None, None, ('kv', 'tp')), may hold values from -0.09375 to 0.09375
- down_weights: bfloat16 [2, 11264, 4096], P(None, ('kv', 'tp')), may hold values from -0.4375 to 0.4375
- norm_gain: bfloat16 [3, 4096], P(None, ('kv', 'tp')), may hold values from 0.25 to 4.5
- norm_bias: bfloat16 [3, 4096], P(None, ('kv', 'tp')), may hold values from -3 to 3
- query_weight: bfloat16 [4096, 4096], P('kv', 'tp'), may hold values from -0.09375 to 0.09375
- forget_weight: bfloat16 [4096, 4096], P('kv', 'tp'), may hold values from -0.09375 to 0.09375
- input_weight: bfloat16 [4096, 4096], P('kv', 'tp'), may hold values from -0.09375 to 0.09375
- outgate_weight: bfloat16 [4096, 4096], P('kv', 'tp'), may hold values from -0.09375 to 0.09375
- lower_bound: float32 [4096], P('tp'), may hold values from 0.05 to 0.9
- head_gain: float32 [4096], P('tp'), may hold values from 0.1 to 1.9
- out_weight: bfloat16 [4096, 4096], P('tp'), may hold values from -0.25 to 0.25
- state: float32 [16, 32, 128, 128], P('kv', 'tp'), may hold values from -3 to 3
Outputs:
- mixed: bfloat16 [16, 4096], P(None, ('kv', 'tp'))
- new_state: float32 [16, 32, 128, 128], P('kv', 'tp')
The draws below stay inside these ranges and needn't reach their ends.
All inputs are finite; a program needn't handle non-finite values.
Results may differ from the reference program's by a relative error of at most 0.022.
Values may be sent and summed in bfloat16 or wider, within the bound.
A program may use at most 64 MiB of HBM per device.

```python
import math
import jax
import jax.numpy as jnp
from jax import lax

D = 4096
FF = 11264
HEAD = 128
HEADS = 32
BATCH = 16


def draw_tokens(key, part):
    position = jnp.arange(D, dtype=jnp.float32)[None, :] / D
    values = jax.random.normal(key, (BATCH, D), jnp.float32) * 0.4 * 4.0 ** position
    return jnp.clip(values, -8.0, 8.0).astype(jnp.bfloat16)


def draw_norm_gain(key, part):
    position = jnp.arange(D, dtype=jnp.float32)[None, :] / D
    jitter = 1.0 + 0.3 * jax.random.uniform(key, (3, D), jnp.float32, -1.0, 1.0)
    values = 0.6 * 3.0 ** position * jitter
    return values.astype(jnp.bfloat16)


def with_spikes(result, own_key, source, target, parts, factor):
    owner, partner = [(jnp.arange(result.shape[dim]) // (result.shape[dim] // parts)).reshape([-1 if axis == dim else 1 for axis in range(result.ndim)]) for dim in (source, target)]
    chosen = jax.random.permutation(own_key, parts)[partner]
    strong = (owner == chosen) | (owner == (partner + parts // 2) % parts)
    return jnp.where(strong, factor * result, result)


def block_scale(key, dims, cuts, least, top_value):
    factor_of, own = 1.0, jax.random.fold_in(key, 6)
    for dim, blocks in cuts:
        steps = jnp.exp(jax.random.uniform(jax.random.fold_in(own, dim), (blocks,), jnp.float32, least / len(cuts), top_value / len(cuts)))
        factor_of = factor_of * jnp.repeat(steps, dims[dim] // blocks).reshape([-1 if axis == dim else 1 for axis in range(len(dims))])
    return factor_of


def noise(rng, shape, scale, bound, cuts=(), held_as=jnp.bfloat16):
    drawn = scale * jax.random.normal(rng, shape, jnp.float32)
    if cuts:
        drawn = drawn * block_scale(rng, shape, cuts, -0.22, 0.18)
    return jnp.clip(drawn, -bound, bound).astype(held_as)


def noise_with(rng, shape, scale, reach, cuts, heavy, held_as=jnp.bfloat16):
    array = scale * jax.random.normal(rng, shape, jnp.float32)
    if cuts:
        array = array * block_scale(rng, shape, cuts, -0.22, 0.18)
    return jnp.clip(with_spikes(array, jax.random.fold_in(rng, 3), *heavy), -reach, reach).astype(held_as)


def setup_inputs(seed: int = 0) -> dict:
    arg_keys = jax.random.split(jax.random.key(seed), 15)
    tokens = draw_tokens(jax.random.fold_in(arg_keys[14], 71), 0)
    gate_weights = noise(arg_keys[1], (2, D, FF), D ** -0.5, 0.09375, ((2, 32),))
    up_weights = noise(arg_keys[2], (2, D, FF), D ** -0.5, 0.09375, ((2, 32),))
    down_weights = noise_with(arg_keys[3], (2, FF, D), (FF // 16) ** -0.5, 0.4375, ((1, 32),), (1, 2, 32, 2.75))
    norm_gain = draw_norm_gain(jax.random.fold_in(arg_keys[14], 71), 0)
    norm_bias = noise(arg_keys[5], (3, D), 0.5, 3.0, ((1, 32),))
    query_weight = noise(arg_keys[6], (D, D), D ** -0.5, 0.09375, ((0, 8), (1, 4)))
    forget_weight = noise(arg_keys[7], (D, D), D ** -0.5, 0.09375, ((0, 8), (1, 4)))
    input_weight = noise(arg_keys[8], (D, D), D ** -0.5, 0.09375, ((0, 8), (1, 4)))
    outgate_weight = noise(arg_keys[9], (D, D), D ** -0.5, 0.09375, ((0, 8), (1, 4)))
    lower_bound = jnp.clip(jnp.exp(math.log(0.9) - 2.8903717 * jax.random.uniform(arg_keys[10], (D,), jnp.float32) ** block_scale(arg_keys[10], (D,), ((0, 4),), -0.2, 0.2)), 0.05, 0.9)
    head_gain = jnp.clip(1.0 + 0.18 * jax.random.normal(arg_keys[11], (D,), jnp.float32), 0.1, 1.9)
    out_weight = noise_with(arg_keys[12], (D, D), (D // 4) ** -0.5, 0.25, ((0, 4),), (0, 1, 4, 2.0))
    state = noise(arg_keys[13], (BATCH, HEADS, HEAD, HEAD), 0.5, 3.0, ((0, 8), (1, 4)), jnp.float32)
    return {"tokens": tokens, "gate_weights": gate_weights, "up_weights": up_weights, "down_weights": down_weights, "norm_gain": norm_gain, "norm_bias": norm_bias, "query_weight": query_weight, "forget_weight": forget_weight, "input_weight": input_weight, "outgate_weight": outgate_weight, "lower_bound": lower_bound, "head_gain": head_gain, "out_weight": out_weight, "state": state}


residual_scale = 8.0 ** 0.25
norm_eps = 1e-05
head_eps = 1e-06

def layer_norm(stream, gain_row, bias_row):
    row_mean = lax.optimization_barrier(jnp.mean(stream, axis=-1, keepdims=True))
    centred = stream - row_mean
    spread = lax.optimization_barrier(jnp.mean(centred * centred, axis=-1, keepdims=True))
    return centred * lax.rsqrt(spread + norm_eps) * gain_row.astype(jnp.float32) + bias_row.astype(jnp.float32)

def half_ffn(row_block, gate_w, up_w, down_w):
    gate_proj = jnp.dot(row_block, gate_w, preferred_element_type=jnp.float32)
    up_proj = jnp.dot(row_block, up_w, preferred_element_type=jnp.float32)
    hidden = (jax.nn.silu(gate_proj) * up_proj).astype(jnp.bfloat16)
    return jnp.dot(hidden, down_w, preferred_element_type=jnp.float32)

def reference(tokens, gate_weights, up_weights, down_weights, norm_gain, norm_bias, query_weight, forget_weight, input_weight, outgate_weight, lower_bound, head_gain, out_weight, state):
    head_count = D // HEAD
    row_count = tokens.shape[0]
    branch_one = half_ffn(tokens, gate_weights[0], up_weights[0], down_weights[0])
    stream = residual_scale * tokens.astype(jnp.float32) + 0.5 * branch_one
    normed = layer_norm(stream, norm_gain[0], norm_bias[0]).astype(jnp.bfloat16)
    projected = [jnp.dot(normed, weight, preferred_element_type=jnp.float32).astype(jnp.bfloat16) for weight in (query_weight, forget_weight, input_weight, outgate_weight)]
    shaped = [piece_pre.astype(jnp.float32).reshape(row_count, head_count, HEAD) for piece_pre in projected[:3]]
    low_bound = lower_bound.reshape(head_count, HEAD)

    def one_sequence(pieces):
        query_pre, forget_pre, input_pre, old_state = pieces
        forget = low_bound + (1.0 - low_bound) * jax.nn.sigmoid(forget_pre)
        key_part = (1.0 - low_bound) * jax.nn.sigmoid(-forget_pre)
        updated = forget[:, :, None] * old_state + key_part[:, :, None] * input_pre[:, None, :]
        readout = jnp.einsum('hd,hde->he', jax.nn.silu(query_pre), updated, precision=lax.Precision.HIGHEST)
        return (readout, updated)
    readout, new_state = lax.map(one_sequence, (shaped[0], shaped[1], shaped[2], state))
    readout = readout * lax.rsqrt(lax.optimization_barrier(jnp.mean(readout * readout, axis=-1, keepdims=True)) + head_eps)
    gated_out = (readout.reshape(row_count, D) * head_gain * jax.nn.silu(projected[3].astype(jnp.float32))).astype(jnp.bfloat16)
    mixed_out = jnp.dot(gated_out, out_weight, preferred_element_type=jnp.float32)
    stream = (residual_scale * normed.astype(jnp.float32) + mixed_out).astype(jnp.bfloat16)
    normed = layer_norm(stream.astype(jnp.float32), norm_gain[1], norm_bias[1]).astype(jnp.bfloat16)
    branch_two = half_ffn(normed, gate_weights[1], up_weights[1], down_weights[1])
    stream = residual_scale * normed.astype(jnp.float32) + 0.5 * branch_two
    mixed = layer_norm(stream, norm_gain[2], norm_bias[2]).astype(jnp.bfloat16)
    return (mixed, new_state)
```

```python
import functools

import jax
import jax.numpy as jnp
from jax import lax
from jax.experimental import pallas as pl
from jax.experimental.pallas import tpu as pltpu
from jax.sharding import PartitionSpec as P

MESH = pl.DeviceIdType.MESH

HEAD = 128


residual_scale = 8.0**0.25
norm_eps = 1e-05
head_eps = 1e-06


def whole_norm(stream, gain_row, bias_row):
    row_mean = jnp.mean(stream, axis=-1, keepdims=True)
    centred = stream - row_mean
    spread = jnp.mean(centred * centred, axis=-1, keepdims=True)
    return centred * lax.rsqrt(spread + norm_eps) * gain_row.astype(jnp.float32) + bias_row.astype(
        jnp.float32
    )


def ffn_partial(whole_rows, gate_w, up_w, down_w):
    gate_proj = jnp.dot(whole_rows, gate_w, preferred_element_type=jnp.float32)
    up_proj = jnp.dot(whole_rows, up_w, preferred_element_type=jnp.float32)
    hidden = (jax.nn.silu(gate_proj) * up_proj).astype(jnp.bfloat16)
    return jnp.dot(hidden, down_w, preferred_element_type=jnp.float32)


def local(
    tokens,
    gate_weights,
    up_weights,
    down_weights,
    norm_gain,
    norm_bias,
    query_weight,
    forget_weight,
    input_weight,
    outgate_weight,
    lower_bound,
    head_gain,
    out_weight,
    state,
):
    own_cols = tokens.shape[1]
    col_offset = lax.axis_index(("kv", "tp")) * own_cols
    whole_tokens, whole_gain, whole_bias = (
        lax.all_gather(tokens, ("kv", "tp"), axis=1, tiled=True),
        lax.all_gather(norm_gain, ("kv", "tp"), axis=1, tiled=True),
        lax.all_gather(norm_bias, ("kv", "tp"), axis=1, tiled=True),
    )

    def finish(partial_value, residual_whole, index, want_whole):
        total = lax.psum(partial_value, ("kv", "tp"))
        stream = residual_scale * residual_whole + 0.5 * total
        normed = whole_norm(stream, whole_gain[index], whole_bias[index]).astype(jnp.bfloat16)
        if want_whole:
            return normed
        return lax.dynamic_slice_in_dim(normed, col_offset, own_cols, 1)

    partial_one = ffn_partial(whole_tokens, gate_weights[0], up_weights[0], down_weights[0])
    normed_one = finish(partial_one, whole_tokens.astype(jnp.float32), 0, True)
    seq_count = state.shape[0]
    head_count = state.shape[1]
    head_cols = query_weight.shape[1]
    weight_rows = query_weight.shape[0]
    seq_offset = lax.axis_index("kv") * seq_count
    block_rows = lax.dynamic_slice_in_dim(
        normed_one, lax.axis_index("kv") * weight_rows, weight_rows, 1
    )
    weights = (query_weight, forget_weight, input_weight, outgate_weight)
    projected = lax.psum_scatter(
        jnp.concatenate(
            [jnp.dot(block_rows, weight, preferred_element_type=jnp.float32) for weight in weights],
            axis=1,
        ).astype(jnp.bfloat16),
        "kv",
        scatter_dimension=0,
        tiled=True,
    )
    query_pre = projected[:, :head_cols].astype(jnp.float32).reshape(seq_count, head_count, HEAD)
    forget_pre = (
        projected[:, head_cols : 2 * head_cols]
        .astype(jnp.float32)
        .reshape(seq_count, head_count, HEAD)
    )
    input_pre = (
        projected[:, 2 * head_cols : 3 * head_cols]
        .astype(jnp.float32)
        .reshape(seq_count, head_count, HEAD)
    )
    outgate_pre = projected[:, 3 * head_cols :].astype(jnp.float32)
    low_bound = lower_bound.reshape(head_count, HEAD)
    forget = low_bound + (1.0 - low_bound) * jax.nn.sigmoid(forget_pre)
    key_part = (1.0 - low_bound) * jax.nn.sigmoid(-forget_pre)
    updated = forget[..., None] * state + key_part[..., None] * input_pre[:, :, None, :]
    readout = jnp.einsum(
        "shd,shde->she", jax.nn.silu(query_pre), updated, precision=lax.Precision.HIGHEST
    )
    readout = readout * lax.rsqrt(jnp.mean(readout * readout, axis=-1, keepdims=True) + head_eps)
    gated_out = (
        readout.reshape(seq_count, head_cols) * head_gain * jax.nn.silu(outgate_pre)
    ).astype(jnp.bfloat16)
    mixer_part = jnp.dot(gated_out, out_weight, preferred_element_type=jnp.float32)
    head_sum = lax.psum_scatter(
        mixer_part.astype(jnp.bfloat16), "tp", scatter_dimension=1, tiled=True
    ).astype(jnp.float32)
    piece_cols = head_sum.shape[1]
    own_normed = lax.dynamic_slice_in_dim(normed_one, seq_offset, seq_count, 0)
    own_normed = lax.dynamic_slice_in_dim(
        own_normed, lax.axis_index("tp") * piece_cols, piece_cols, 1
    )
    stream_own = (residual_scale * own_normed.astype(jnp.float32) + head_sum).astype(jnp.bfloat16)
    seq_rows = lax.all_gather(stream_own, "tp", axis=1, tiled=True)
    stream_two = lax.all_gather(seq_rows, "kv", axis=0, tiled=True)
    normed_two = whole_norm(stream_two.astype(jnp.float32), whole_gain[1], whole_bias[1]).astype(
        jnp.bfloat16
    )
    partial_two = ffn_partial(normed_two, gate_weights[1], up_weights[1], down_weights[1])
    mixed = finish(partial_two, normed_two.astype(jnp.float32), 2, False)
    return (mixed, updated)


KINDS = ("gb", "rs_one", "turn", "own_tp", "base", "rs_three", "spread")


def tree_sum(terms):
    while len(terms) > 1:
        rest = [terms[-1]] if len(terms) % 2 else []
        terms = [a + b for a, b in zip(terms[::2], terms[1::2])] + rest
    return terms[0]


def total_of(tiles):
    rows = jnp.sum(tree_sum(tiles), axis=0, keepdims=True)
    return jnp.sum(rows, axis=1, keepdims=True)


def dot_turned(rows, weights):
    return lax.dot_general(
        rows, weights, (((1,), (1,)), ((), ())), preferred_element_type=jnp.float32
    )


def flipped(value, count, mask):
    out, bit = value, 1
    while bit < count:
        if mask & bit:
            out = out + bit - 2 * bit * lax.rem(lax.div(value, bit), 2)
        bit *= 2
    return out


def layer_kernel(
    n_kv,
    n_tp,
    tokens_hbm,
    gain_hbm,
    bias_hbm,
    low_hbm,
    head_gain_hbm,
    gate_hbm,
    up_hbm,
    down_hbm,
    query_hbm,
    forget_hbm,
    input_hbm,
    outgate_hbm,
    out_hbm,
    state_hbm,
    mixed_ref,
    state_out,
    gate_v,
    up_v,
    down_v,
    proj_v,
    out_v,
    state_v,
    new_v,
    gain_v,
    bias_v,
    low_v,
    head_gain_v,
    tok_buf,
    gb_buf,
    rs_send,
    rs_recv_one,
    rs_recv_three,
    turn_send,
    turn_recv,
    own_tp,
    base_f32,
    base_send,
    base_recv,
    proj_f32,
    proj_send,
    proj_recv,
    gated_buf,
    head_f32,
    head_buf,
    ag_two,
    ag_two_f32,
    normed_bf,
    spread_buf,
    final_buf,
    send_sem,
    recv_sem,
    tok_sem,
    proj_sem,
    head_sem,
    ag_sem,
    load_sem,
    store_sem,
):
    n = n_kv * n_tp
    batch, lane = tok_buf.shape[1:]
    width = n * lane
    seqs, heads = state_v.shape[0], state_v.shape[1]
    part_rows = ag_two.shape[2]
    per = part_rows // seqs
    parts = n // per
    group = n_tp * lane
    bf16, f32 = jnp.bfloat16, jnp.float32
    kv, tp = lax.axis_index("kv"), lax.axis_index("tp")
    me = kv * n_tp + tp
    kv_of = [flipped(kv, n_kv, m) for m in range(n_kv)]
    tp_of = [flipped(tp, n_tp, m) for m in range(n_tp)]
    peers = [(k, t) for k in reversed(range(n_kv)) for t in reversed(range(n_tp)) if k or t]

    barrier = pltpu.get_barrier_semaphore()
    for k, t in peers:
        pl.semaphore_signal(
            barrier, inc=1, device_id=(kv_of[k], tp_of[t]), device_id_type=MESH
        )

    proj_hbm = (query_hbm, forget_hbm, input_hbm, outgate_hbm)
    loads = {}
    order = [("tokens", tokens_hbm, tok_buf.at[me])]
    order += [("gain", gain_hbm, gain_v), ("bias", bias_hbm, bias_v)]
    order += [("gate0", gate_hbm.at[0], gate_v.at[0]), ("up0", up_hbm.at[0], up_v.at[0])]
    order += [("down0", down_hbm.at[0], down_v.at[0])]
    order += [("proj%d" % i, proj_hbm[i], proj_v.at[i]) for i in range(4)]
    order += [("low", low_hbm, low_v), ("head_gain", head_gain_hbm, head_gain_v)]
    order += [("state", state_hbm, state_v), ("out", out_hbm, out_v)]
    order += [("gate1", gate_hbm.at[1], gate_v.at[1]), ("up1", up_hbm.at[1], up_v.at[1])]
    order += [("down1", down_hbm.at[1], down_v.at[1])]
    for i, (name, source, target) in enumerate(order):
        loads[name] = pltpu.make_async_copy(source, target, load_sem.at[i])
        loads[name].start()

    def send(src, dst, kind, recv, k, t):
        pltpu.make_async_remote_copy(
            src_ref=src,
            dst_ref=dst,
            send_sem=send_sem.at[kind],
            recv_sem=recv,
            device_id=(kv_of[k], tp_of[t]),
            device_id_type=MESH,
        ).start()

    def wait_for(sem, ref, count):
        part = ref.at[pl.ds(0, count)]
        pltpu.make_async_copy(part, part, sem).wait()

    GB, RS_ONE, TURN, OWN_TP, BASE, RS_THREE, SPREAD = range(len(KINDS))
    TOK, PROJ, HEADS_SUM, AG_TWO = range(len(KINDS), len(KINDS) + 4)

    loads["gain"].wait()
    loads["bias"].wait()
    pad = jnp.zeros((2, lane), f32)
    gains = jnp.concatenate([gain_v[...].astype(f32), bias_v[...].astype(f32), pad], axis=0)
    gb_buf[me] = gains
    loads["tokens"].wait()
    pl.semaphore_wait(barrier, n - 1)
    for k, t in peers:
        send(tok_buf.at[me], tok_buf.at[me], TOK, tok_sem.at[kv], k, t)
    for k, t in peers:
        send(gb_buf.at[me], gb_buf.at[me], GB, recv_sem.at[GB], k, t)

    def columns(index, size):
        return pl.ds(pl.multiple_of(index * size, size), size)

    def hidden_of(gate, up):
        return (jax.nn.silu(gate) * up).astype(bf16)

    def reduce_scatter_start(hidden, layer, kind, recv):
        loads["down%d" % layer].wait()
        for k in reversed(range(n_kv)):
            target = kv_of[k]
            part = jnp.dot(
                hidden, down_v[layer, :, columns(target, group)], preferred_element_type=f32
            ).astype(bf16)
            for t in range(n_tp):
                rs_send[target * n_tp + t] = part[:, t * lane : (t + 1) * lane]
            for t in reversed(range(n_tp)):
                if k or t:
                    index = target * n_tp + tp_of[t]
                    send(rs_send.at[index], recv.at[me], kind, recv_sem.at[kind], k, t)
        recv[me] = rs_send[me]

    def reduce_scatter_end(kind, recv):
        wait_for(recv_sem.at[kind], recv, n - 1)
        return tree_sum([recv[j].astype(f32) for j in range(n)])

    gate = up = None
    for k in range(n_kv):
        source = kv_of[k]
        wait_for(tok_sem.at[source], tok_buf, n_tp if k else n_tp - 1)
        rows = jnp.concatenate([tok_buf[source * n_tp + t] for t in range(n_tp)], axis=1)
        cols = columns(source, group)
        if k == 0:
            loads["gate0"].wait()
            loads["up0"].wait()
        gate_part = dot_turned(rows, gate_v[0, :, cols])
        up_part = dot_turned(rows, up_v[0, :, cols])
        gate = gate_part if gate is None else gate + gate_part
        up = up_part if up is None else up + up_part
    reduce_scatter_start(hidden_of(gate, up), 0, RS_ONE, rs_recv_one)

    token_sum = jnp.sum(
        tree_sum([tok_buf[j].astype(f32) for j in range(n)]), axis=1, keepdims=True
    )
    centre = residual_scale * token_sum / width
    own_tokens = residual_scale * tok_buf[me].astype(f32) - centre

    wait_for(recv_sem.at[GB], gb_buf, n - 1)
    kv_gains = jnp.concatenate([gb_buf[kv * n_tp + t] for t in range(n_tp)], axis=1).astype(bf16)
    for i in range(4):
        loads["proj%d" % i].wait()
        based = jnp.dot(kv_gains, proj_v[i], preferred_element_type=f32)
        for h in range(heads):
            block = slice(h * HEAD, (h + 1) * HEAD)
            base_f32[i, h : h + 1, :] = based[0:1, block]
            base_f32[i, heads + h : heads + h + 1, :] = based[3:4, block]
    base_send[...] = base_f32[...].astype(bf16)
    for k in reversed(range(1, n_kv)):
        send(base_send, base_recv.at[kv], BASE, recv_sem.at[BASE], k, 0)
    base_recv[kv] = base_send[...]

    shifted = own_tokens + 0.5 * reduce_scatter_end(RS_ONE, rs_recv_one)
    own_tp[tp] = (shifted * gains[0:1, :]).astype(bf16)
    for t in reversed(range(1, n_tp)):
        send(own_tp.at[tp], own_tp.at[tp], OWN_TP, recv_sem.at[OWN_TP], 0, t)
    for j in range(n_kv):
        turn_send[j] = shifted[j * seqs : (j + 1) * seqs, :]
    for k, t in peers:
        send(turn_send.at[kv_of[k]], turn_recv.at[me], TURN, recv_sem.at[TURN], k, t)
    turn_recv[me] = turn_send[kv]

    wait_for(recv_sem.at[OWN_TP], own_tp, n_tp - 1)
    block = jnp.concatenate([own_tp[t] for t in range(n_tp)], axis=1)
    turns = (1, 2, 0, 3)
    for i in turns:
        part = jnp.dot(block, proj_v[i], preferred_element_type=f32)
        for h in range(heads):
            for r in range(0, batch, 8):
                proj_f32[i, pl.ds(r * heads + h, 8, stride=heads), :] = part[
                    r : r + 8, h * HEAD : (h + 1) * HEAD
                ]
        proj_send[i] = proj_f32[i].reshape(proj_send.shape[1:]).astype(bf16)
        for k in reversed(range(1, n_kv)):
            send(proj_send.at[i, kv_of[k]], proj_recv.at[i, kv], PROJ, proj_sem.at[i], k, 0)
        proj_recv[i, kv] = proj_send[i, kv]

    wait_for(recv_sem.at[BASE], base_recv, n_kv - 1)
    base = tree_sum([base_recv[j].astype(f32) for j in range(n_kv)])
    wait_for(recv_sem.at[TURN], turn_recv, n - 1)

    def gain_rows(c, index):
        return gb_buf[c * per : (c + 1) * per, index, :]

    def norm_rows(tiles, index):
        mean = total_of(tiles) / width
        centred = [tile - mean for tile in tiles]
        scale = lax.rsqrt(total_of([c * c for c in centred]) / width + norm_eps)
        normed = [
            (tile * scale * gain_rows(c, index) + gain_rows(c, 3 + index)).astype(bf16)
            for c, tile in enumerate(centred)
        ]
        return mean, scale, normed

    norm_one = [
        norm_rows([turn_recv[c * per : (c + 1) * per, s, :] for c in range(parts)], 0)
        for s in range(seqs)
    ]
    residual = [
        [residual_scale * tile.astype(f32) for tile in norm_one[s][2]] for s in range(seqs)
    ]

    def projected(i):
        wait_for(proj_sem.at[i], proj_recv.at[i], n_kv - 1)
        total = tree_sum([proj_recv[i, j].astype(f32) for j in range(n_kv)])
        found = []
        for s in range(seqs):
            mean, scale, _ = norm_one[s]
            rows = total[s * heads : (s + 1) * heads] - mean * base[i, 0:heads]
            rows = scale * rows + base[i, heads : 2 * heads]
            found.append(rows.astype(bf16).astype(f32))
        return found

    loads["low"].wait()
    low = low_v[...]
    forget_pre = projected(1)
    forget = [low + (1.0 - low) * jax.nn.sigmoid(p) for p in forget_pre]
    key_part = [(1.0 - low) * jax.nn.sigmoid(-p) for p in forget_pre]
    input_pre = projected(2)
    query = [jax.nn.silu(p) for p in projected(0)]
    fill = jnp.zeros((HEAD - 3 * seqs * heads, HEAD), f32)
    seen = [q * f for q, f in zip(query, forget)]
    turned = jnp.concatenate([*seen, *forget, *key_part, fill], axis=0).T

    def column(kind, s, h):
        first = (kind * seqs + s) * heads + h
        return turned[:, first : first + 1]

    loads["state"].wait()
    readouts = []
    for s in range(seqs):
        rows = [
            jnp.sum(column(0, s, h) * state_v[s, h], axis=0, keepdims=True) for h in range(heads)
        ]
        match = jnp.sum(query[s] * key_part[s], axis=1, keepdims=True)
        readout = jnp.concatenate(rows, axis=0) + match * input_pre[s]
        mean_square = jnp.mean(readout * readout, axis=1, keepdims=True)
        readouts.append(readout * lax.rsqrt(mean_square + head_eps))
    loads["head_gain"].wait()
    outgate = projected(3)
    for s in range(seqs):
        gated_buf[s * heads : (s + 1) * heads, :] = (
            readouts[s] * head_gain_v[...] * jax.nn.silu(outgate[s])
        )
    gated = jnp.concatenate(
        [gated_buf[pl.ds(h, seqs, stride=heads), :] for h in range(heads)], axis=1
    ).astype(bf16)
    loads["out"].wait()
    step = per * lane
    for c in range(parts):
        part = jnp.dot(gated, out_v[:, c * step : (c + 1) * step], preferred_element_type=f32)
        for j in range(per):
            head_f32[c, pl.ds(j, seqs, stride=per), :] = part[:, j * lane : (j + 1) * lane]
        head_buf[c, tp] = head_f32[c].astype(bf16)
        for t in reversed(range(1, n_tp)):
            send(head_buf.at[c, tp], head_buf.at[c, tp], HEADS_SUM, head_sem.at[c], 0, t)

    for s in range(seqs):
        for h in range(heads):
            new_v[s, h] = (
                column(1, s, h) * state_v[s, h] + column(2, s, h) * input_pre[s][h : h + 1, :]
            )
    store = pltpu.make_async_copy(new_v, state_out, store_sem)
    store.start()

    streams = [[] for _ in range(seqs)]
    for c in range(parts):
        wait_for(head_sem.at[c], head_buf.at[c], n_tp - 1)
        head_total = tree_sum([head_buf[c, t].astype(f32) for t in range(n_tp)])
        for s in range(seqs):
            mixed_rows = residual[s][c] + head_total[s * per : (s + 1) * per]
            streams[s].append(mixed_rows.astype(bf16).astype(f32))
    norm_two = [norm_rows(streams[s], 1)[2] for s in range(seqs)]
    for c in range(parts):
        ag_two[c, kv] = jnp.concatenate([norm_two[s][c] for s in range(seqs)], axis=0)
        for k in reversed(range(1, n_kv)):
            send(ag_two.at[c, kv], ag_two.at[c, kv], AG_TWO, ag_sem.at[c], k, 0)

    wait_for(send_sem.at[RS_ONE], rs_recv_one, n - 1)
    loads["gate1"].wait()
    loads["up1"].wait()
    gate = up = None
    for c in range(parts):
        wait_for(ag_sem.at[c], ag_two.at[c], n_kv - 1)
        ag_two_f32[c] = ag_two[c].astype(f32).reshape(ag_two_f32.shape[1:])
        tiles = []
        for j in range(per):
            pieces = [
                ag_two_f32[c, pl.ds(s * per + j, n_kv, stride=part_rows), :] for s in range(seqs)
            ]
            tiles.append(jnp.concatenate(pieces, axis=0).astype(bf16))
            normed_bf[c * per + j] = tiles[-1]
        rows = jnp.concatenate(tiles, axis=1)
        cols = slice(c * step, (c + 1) * step)
        gate_part = dot_turned(rows, gate_v[1, :, cols])
        up_part = dot_turned(rows, up_v[1, :, cols])
        gate = gate_part if gate is None else gate + gate_part
        up = up_part if up is None else up + up_part
    reduce_scatter_start(hidden_of(gate, up), 1, RS_THREE, rs_recv_three)
    own_rows = residual_scale * normed_bf[me].astype(f32)

    row_ids = lax.broadcasted_iota(jnp.int32, (batch, lane), 0)
    lane_ids = lax.broadcasted_iota(jnp.int32, (batch, lane), 1)
    stream = own_rows + 0.5 * reduce_scatter_end(RS_THREE, rs_recv_three)
    own_mean = jnp.sum(stream, axis=1, keepdims=True) / lane
    own_centred = stream - own_mean
    own_spread = jnp.sum(own_centred * own_centred, axis=1, keepdims=True)

    def to_lanes(values):
        return jnp.sum(jnp.where(row_ids == lane_ids, values, 0.0), axis=0, keepdims=True)

    spread_buf[me] = jnp.concatenate([to_lanes(own_mean), to_lanes(own_spread)], axis=0)
    for k, t in peers:
        send(spread_buf.at[me], spread_buf.at[me], SPREAD, recv_sem.at[SPREAD], k, t)

    for s in range(seqs):
        final_buf[pl.ds(s, n_kv, stride=seqs), :] = stream[s * n_kv : (s + 1) * n_kv, :]
    natural = final_buf[...]
    for kind in (TOK, RS_THREE):
        wait_for(send_sem.at[kind], tok_buf, n - 1)
    wait_for(send_sem.at[GB], gb_buf, n - 1)
    wait_for(send_sem.at[TURN], turn_recv, n - 1)
    wait_for(send_sem.at[OWN_TP], own_tp, n_tp - 1)
    wait_for(send_sem.at[BASE], base_recv, n_kv - 1)
    for i in range(4):
        wait_for(send_sem.at[PROJ], proj_recv.at[i], n_kv - 1)
    for c in range(parts):
        wait_for(send_sem.at[HEADS_SUM], head_buf.at[c], n_tp - 1)
        wait_for(send_sem.at[AG_TWO], ag_two.at[c], n_kv - 1)
    store.wait()

    wait_for(recv_sem.at[SPREAD], spread_buf, n - 1)
    means = spread_buf[:, 0, :]
    mean_row = jnp.sum(means, axis=0, keepdims=True) / n
    apart = means - mean_row
    square_row = jnp.sum(spread_buf[:, 1, :] + lane * (apart * apart), axis=0, keepdims=True)
    scale_row = lax.rsqrt(square_row / width + norm_eps)
    place = lax.rem(row_ids, seqs) * n_kv + lax.div(row_ids, seqs)

    def to_rows(values):
        return jnp.sum(jnp.where(place == lane_ids, values, 0.0), axis=1, keepdims=True)

    mixed = (natural - to_rows(mean_row)) * to_rows(scale_row) * gains[2:3, :] + gains[5:6, :]
    mixed_ref[...] = mixed.astype(bf16)
    wait_for(send_sem.at[SPREAD], spread_buf, n - 1)


def fused(n_kv, n_tp, *args):
    (
        tokens,
        gate_weights,
        up_weights,
        down_weights,
        norm_gain,
        norm_bias,
        query_weight,
        forget_weight,
        input_weight,
        outgate_weight,
        lower_bound,
        head_gain,
        out_weight,
        state,
    ) = args
    batch, lane = tokens.shape
    n = n_kv * n_tp
    seqs, heads = state.shape[:2]
    gate_weights = jnp.swapaxes(gate_weights, 1, 2)
    up_weights = jnp.swapaxes(up_weights, 1, 2)
    bf16, f32 = jnp.bfloat16, jnp.float32
    per = 8
    parts, part_rows = n // per, per * seqs
    seq_rows = seqs * heads
    scratch = [
        pltpu.VMEM(gate_weights.shape, bf16),
        pltpu.VMEM(up_weights.shape, bf16),
        pltpu.VMEM(down_weights.shape, bf16),
        pltpu.VMEM((4, *query_weight.shape), bf16),
        pltpu.VMEM(out_weight.shape, bf16),
        pltpu.VMEM(state.shape, f32),
        pltpu.VMEM(state.shape, f32),
        pltpu.VMEM(norm_gain.shape, bf16),
        pltpu.VMEM(norm_bias.shape, bf16),
        pltpu.VMEM((heads, HEAD), f32),
        pltpu.VMEM((heads, HEAD), f32),
        pltpu.VMEM((n, batch, lane), bf16),
        pltpu.VMEM((n, 8, lane), f32),
        pltpu.VMEM((n, batch, lane), bf16),
        pltpu.VMEM((n, batch, lane), bf16),
        pltpu.VMEM((n, batch, lane), bf16),
        pltpu.VMEM((n_kv, seqs, lane), f32),
        pltpu.VMEM((n, seqs, lane), f32),
        pltpu.VMEM((n_tp, batch, lane), bf16),
        pltpu.VMEM((4, 2 * heads, HEAD), f32),
        pltpu.VMEM((4, 2 * heads, HEAD), bf16),
        pltpu.VMEM((n_kv, 4, 2 * heads, HEAD), bf16),
        pltpu.VMEM((4, batch * heads, HEAD), f32),
        pltpu.VMEM((4, n_kv, seq_rows, HEAD), bf16),
        pltpu.VMEM((4, n_kv, seq_rows, HEAD), bf16),
        pltpu.VMEM((seq_rows, HEAD), f32),
        pltpu.VMEM((parts, part_rows, lane), f32),
        pltpu.VMEM((parts, n_tp, part_rows, lane), bf16),
        pltpu.VMEM((parts, n_kv, part_rows, lane), bf16),
        pltpu.VMEM((parts, n_kv * part_rows, lane), f32),
        pltpu.VMEM((n, batch, lane), bf16),
        pltpu.VMEM((n, 2, lane), f32),
        pltpu.VMEM((batch, lane), f32),
        pltpu.SemaphoreType.DMA((len(KINDS) + 4,)),
        pltpu.SemaphoreType.DMA((len(KINDS),)),
        pltpu.SemaphoreType.DMA((n_kv,)),
        pltpu.SemaphoreType.DMA((4,)),
        pltpu.SemaphoreType.DMA((parts,)),
        pltpu.SemaphoreType.DMA((parts,)),
        pltpu.SemaphoreType.DMA((17,)),
        pltpu.SemaphoreType.DMA,
    ]
    vmem = pl.BlockSpec(memory_space=pltpu.VMEM)
    hbm = pl.BlockSpec(memory_space=pl.ANY)
    return pl.pallas_call(
        functools.partial(layer_kernel, n_kv, n_tp),
        out_shape=(
            jax.ShapeDtypeStruct(tokens.shape, bf16),
            jax.ShapeDtypeStruct(state.shape, f32),
        ),
        in_specs=[hbm] * 14,
        out_specs=(vmem, hbm),
        scratch_shapes=scratch,
        compiler_params=pltpu.CompilerParams(
            collective_id=0, has_side_effects=True, vmem_limit_bytes=60 * 1024 * 1024
        ),
        name="layer",
    )(
        tokens,
        norm_gain,
        norm_bias,
        lower_bound.reshape(heads, HEAD),
        head_gain.reshape(heads, HEAD),
        gate_weights,
        up_weights,
        down_weights,
        query_weight,
        forget_weight,
        input_weight,
        outgate_weight,
        out_weight,
        state,
    )


def power_of_two(count):
    return count & (count - 1) == 0


def dispatch(n_kv, n_tp, *args):
    tokens, state = args[0], args[13]
    batch, lane = tokens.shape
    seqs, heads = state.shape[:2]
    fits = lane == HEAD and batch == 16 and heads == 8 and seqs == 2 and n_kv == 8
    if fits and power_of_two(n_tp) and n_kv * n_tp % 8 == 0:
        return fused(n_kv, n_tp, *args)
    return local(*args)


def solution(mesh):
    n_kv, n_tp = mesh.shape["kv"], mesh.shape["tp"]
    return jax.shard_map(
        functools.partial(dispatch, n_kv, n_tp),
        mesh=mesh,
        in_specs=(
            P(None, ("kv", "tp")),
            P(None, None, ("kv", "tp")),
            P(None, None, ("kv", "tp")),
            P(None, ("kv", "tp"), None),
            P(None, ("kv", "tp")),
            P(None, ("kv", "tp")),
            P("kv", "tp"),
            P("kv", "tp"),
            P("kv", "tp"),
            P("kv", "tp"),
            P("tp"),
            P("tp"),
            P("tp", None),
            P("kv", "tp", None, None),
        ),
        out_specs=(P(None, ("kv", "tp")), P("kv", "tp", None, None)),
        check_vma=False,
    )
```

```python
import functools

import jax
import jax.numpy as jnp
from jax import lax
from jax.experimental import pallas as pl
from jax.experimental.pallas import tpu as pltpu
from jax.sharding import PartitionSpec as P

MESH = pl.DeviceIdType.MESH

HEAD = 128


residual_scale = 8.0**0.25
norm_eps = 1e-05
head_eps = 1e-06


def whole_norm(stream, gain_row, bias_row):
    row_mean = jnp.mean(stream, axis=-1, keepdims=True)
    centred = stream - row_mean
    spread = jnp.mean(centred * centred, axis=-1, keepdims=True)
    return centred * lax.rsqrt(spread + norm_eps) * gain_row.astype(jnp.float32) + bias_row.astype(
        jnp.float32
    )


def ffn_partial(whole_rows, gate_w, up_w, down_w):
    gate_proj = jnp.dot(whole_rows, gate_w, preferred_element_type=jnp.float32)
    up_proj = jnp.dot(whole_rows, up_w, preferred_element_type=jnp.float32)
    hidden = (jax.nn.silu(gate_proj) * up_proj).astype(jnp.bfloat16)
    return jnp.dot(hidden, down_w, preferred_element_type=jnp.float32)


def local(
    tokens,
    gate_weights,
    up_weights,
    down_weights,
    norm_gain,
    norm_bias,
    query_weight,
    forget_weight,
    input_weight,
    outgate_weight,
    lower_bound,
    head_gain,
    out_weight,
    state,
):
    own_cols = tokens.shape[1]
    col_offset = lax.axis_index(("kv", "tp")) * own_cols
    whole_tokens, whole_gain, whole_bias = (
        lax.all_gather(tokens, ("kv", "tp"), axis=1, tiled=True),
        lax.all_gather(norm_gain, ("kv", "tp"), axis=1, tiled=True),
        lax.all_gather(norm_bias, ("kv", "tp"), axis=1, tiled=True),
    )

    def finish(partial_value, residual_whole, index, want_whole):
        total = lax.psum(partial_value, ("kv", "tp"))
        stream = residual_scale * residual_whole + 0.5 * total
        normed = whole_norm(stream, whole_gain[index], whole_bias[index]).astype(jnp.bfloat16)
        if want_whole:
            return normed
        return lax.dynamic_slice_in_dim(normed, col_offset, own_cols, 1)

    partial_one = ffn_partial(whole_tokens, gate_weights[0], up_weights[0], down_weights[0])
    normed_one = finish(partial_one, whole_tokens.astype(jnp.float32), 0, True)
    seq_count = state.shape[0]
    head_count = state.shape[1]
    head_cols = query_weight.shape[1]
    weight_rows = query_weight.shape[0]
    seq_offset = lax.axis_index("kv") * seq_count
    block_rows = lax.dynamic_slice_in_dim(
        normed_one, lax.axis_index("kv") * weight_rows, weight_rows, 1
    )
    weights = (query_weight, forget_weight, input_weight, outgate_weight)
    projected = lax.psum_scatter(
        jnp.concatenate(
            [jnp.dot(block_rows, weight, preferred_element_type=jnp.float32) for weight in weights],
            axis=1,
        ).astype(jnp.bfloat16),
        "kv",
        scatter_dimension=0,
        tiled=True,
    )
    query_pre = projected[:, :head_cols].astype(jnp.float32).reshape(seq_count, head_count, HEAD)
    forget_pre = (
        projected[:, head_cols : 2 * head_cols]
        .astype(jnp.float32)
        .reshape(seq_count, head_count, HEAD)
    )
    input_pre = (
        projected[:, 2 * head_cols : 3 * head_cols]
        .astype(jnp.float32)
        .reshape(seq_count, head_count, HEAD)
    )
    outgate_pre = projected[:, 3 * head_cols :].astype(jnp.float32)
    low_bound = lower_bound.reshape(head_count, HEAD)
    forget = low_bound + (1.0 - low_bound) * jax.nn.sigmoid(forget_pre)
    key_part = (1.0 - low_bound) * jax.nn.sigmoid(-forget_pre)
    updated = forget[..., None] * state + key_part[..., None] * input_pre[:, :, None, :]
    readout = jnp.einsum(
        "shd,shde->she", jax.nn.silu(query_pre), updated, precision=lax.Precision.HIGHEST
    )
    readout = readout * lax.rsqrt(jnp.mean(readout * readout, axis=-1, keepdims=True) + head_eps)
    gated_out = (
        readout.reshape(seq_count, head_cols) * head_gain * jax.nn.silu(outgate_pre)
    ).astype(jnp.bfloat16)
    mixer_part = jnp.dot(gated_out, out_weight, preferred_element_type=jnp.float32)
    head_sum = lax.psum_scatter(
        mixer_part.astype(jnp.bfloat16), "tp", scatter_dimension=1, tiled=True
    ).astype(jnp.float32)
    piece_cols = head_sum.shape[1]
    own_normed = lax.dynamic_slice_in_dim(normed_one, seq_offset, seq_count, 0)
    own_normed = lax.dynamic_slice_in_dim(
        own_normed, lax.axis_index("tp") * piece_cols, piece_cols, 1
    )
    stream_own = (residual_scale * own_normed.astype(jnp.float32) + head_sum).astype(jnp.bfloat16)
    seq_rows = lax.all_gather(stream_own, "tp", axis=1, tiled=True)
    stream_two = lax.all_gather(seq_rows, "kv", axis=0, tiled=True)
    normed_two = whole_norm(stream_two.astype(jnp.float32), whole_gain[1], whole_bias[1]).astype(
        jnp.bfloat16
    )
    partial_two = ffn_partial(normed_two, gate_weights[1], up_weights[1], down_weights[1])
    mixed = finish(partial_two, normed_two.astype(jnp.float32), 2, False)
    return (mixed, updated)


KINDS = ("gain_tp", "gains", "rs_one", "turn", "turn_tp", "own_tp", "base", "bases", "rs_three", "spread")


def tree_sum(terms):
    while len(terms) > 1:
        rest = [terms[-1]] if len(terms) % 2 else []
        terms = [a + b for a, b in zip(terms[::2], terms[1::2])] + rest
    return terms[0]


def total_of(tiles):
    rows = jnp.sum(tree_sum(tiles), axis=0, keepdims=True)
    return jnp.sum(rows, axis=1, keepdims=True)


def dot_turned(rows, weights):
    return lax.dot_general(
        rows, weights, (((1,), (1,)), ((), ())), preferred_element_type=jnp.float32
    )


def flipped(value, count, mask):
    out, bit = value, 1
    while bit < count:
        if mask & bit:
            out = out + bit - 2 * bit * lax.rem(lax.div(value, bit), 2)
        bit *= 2
    return out


def layer_kernel(
    n_kv,
    n_tp,
    tokens_hbm,
    gain_hbm,
    bias_hbm,
    low_hbm,
    head_gain_hbm,
    gate_hbm,
    up_hbm,
    down_hbm,
    query_hbm,
    forget_hbm,
    input_hbm,
    outgate_hbm,
    out_hbm,
    state_hbm,
    mixed_ref,
    new_v,
    gate_v,
    up_v,
    down_v,
    proj_v,
    out_v,
    state_v,
    gain_v,
    bias_v,
    low_v,
    head_gain_v,
    tok_buf,
    gain_tp,
    gain_buf,
    rs_send,
    rs_recv_one,
    rs_recv_three,
    turn_tp,
    turn_recv,
    own_tp,
    base_send,
    base_recv,
    base_all,
    proj_f32,
    proj_send,
    proj_recv,
    gated_buf,
    head_f32,
    head_buf,
    ag_two,
    ag_two_f32,
    normed_bf,
    spread_buf,
    final_buf,
    send_sem,
    recv_sem,
    tok_sem,
    proj_sem,
    head_sem,
    ag_sem,
    load_sem,
):
    n = n_kv * n_tp
    batch, lane = tok_buf.shape[1:]
    width = n * lane
    seqs, heads = state_v.shape[0], state_v.shape[1]
    part_rows = ag_two.shape[2]
    per = part_rows // seqs
    parts = n // per
    group = n_tp * lane
    bf16, f32 = jnp.bfloat16, jnp.float32
    kv, tp = lax.axis_index("kv"), lax.axis_index("tp")
    me = kv * n_tp + tp
    kv_of = [flipped(kv, n_kv, m) for m in range(n_kv)]
    tp_of = [flipped(tp, n_tp, m) for m in range(n_tp)]
    peers = [(k, t) for k in reversed(range(n_kv)) for t in reversed(range(n_tp)) if k or t]

    barrier = pltpu.get_barrier_semaphore()
    for k, t in peers:
        pl.semaphore_signal(
            barrier, inc=1, device_id=(kv_of[k], tp_of[t]), device_id_type=MESH
        )

    proj_hbm = (query_hbm, forget_hbm, input_hbm, outgate_hbm)
    loads = {}
    order = [("tokens", tokens_hbm, tok_buf.at[me])]
    order += [("gain", gain_hbm, gain_v), ("bias", bias_hbm, bias_v)]
    order += [("gate0", gate_hbm.at[0], gate_v.at[0]), ("up0", up_hbm.at[0], up_v.at[0])]
    order += [("down0", down_hbm.at[0], down_v.at[0])]
    order += [("proj%d" % i, proj_hbm[i], proj_v.at[i]) for i in range(4)]
    order += [("low", low_hbm, low_v), ("head_gain", head_gain_hbm, head_gain_v)]
    order += [("state", state_hbm, state_v), ("out", out_hbm, out_v)]
    order += [("gate1", gate_hbm.at[1], gate_v.at[1]), ("up1", up_hbm.at[1], up_v.at[1])]
    order += [("down1", down_hbm.at[1], down_v.at[1])]
    for i, (name, source, target) in enumerate(order):
        loads[name] = pltpu.make_async_copy(source, target, load_sem.at[i])
        if i < 10:
            loads[name].start()

    def send(src, dst, kind, recv, k, t):
        pltpu.make_async_remote_copy(
            src_ref=src,
            dst_ref=dst,
            send_sem=send_sem.at[kind],
            recv_sem=recv,
            device_id=(kv_of[k], tp_of[t]),
            device_id_type=MESH,
        ).start()

    def wait_for(sem, ref, count):
        part = ref.at[pl.ds(0, count)]
        pltpu.make_async_copy(part, part, sem).wait()

    GAIN_TP, GAINS, RS_ONE, TURN, TURN_TP, OWN_TP, BASE, BASES, RS_THREE, SPREAD = range(len(KINDS))
    TOK, PROJ, HEADS_SUM, AG_TWO = range(len(KINDS), len(KINDS) + 4)

    loads["gain"].wait()
    loads["bias"].wait()
    pad = jnp.zeros((2, lane), f32)
    gains, biases = gain_v[...].astype(f32), bias_v[...].astype(f32)
    gains = jnp.concatenate([gains[0:2], biases[0:2], gains[2:3], biases[2:3], pad], axis=0)
    gain_tp[tp] = gains
    loads["tokens"].wait()
    pl.semaphore_wait(barrier, n - 1)
    for k, t in peers:
        send(tok_buf.at[me], tok_buf.at[me], TOK, tok_sem.at[kv], k, t)
    for t in reversed(range(1, n_tp)):
        send(gain_tp.at[tp], gain_tp.at[tp], GAIN_TP, recv_sem.at[GAIN_TP], 0, t)

    for name in [entry[0] for entry in order[10:]]:
        loads[name].start()

    def columns(index, size):
        return pl.ds(pl.multiple_of(index * size, size), size)

    def hidden_of(gate, up):
        return (jax.nn.silu(gate) * up).astype(bf16)

    def reduce_scatter_start(hidden, layer, kind, recv):
        loads["down%d" % layer].wait()
        for k in reversed(range(n_kv)):
            target = kv_of[k]
            part = jnp.dot(
                hidden, down_v[layer, :, columns(target, group)], preferred_element_type=f32
            ).astype(bf16)
            for t in range(n_tp):
                rs_send[target * n_tp + t] = part[:, t * lane : (t + 1) * lane]
            for t in reversed(range(n_tp)):
                if k or t:
                    index = target * n_tp + tp_of[t]
                    send(rs_send.at[index], recv.at[me], kind, recv_sem.at[kind], k, t)
        recv[me] = rs_send[me]

    def reduce_scatter_end(kind, recv):
        wait_for(recv_sem.at[kind], recv, n - 1)
        return tree_sum([recv[j].astype(f32) for j in range(n)])

    def send_bases():
        wait_for(recv_sem.at[GAIN_TP], gain_tp, n_tp - 1)
        for t in range(n_tp):
            gain_buf[kv * n_tp + t] = gain_tp[t, 0:4]
        own_gains = gain_tp.at[:, pl.ds(0, 4)]
        for k in reversed(range(1, n_kv)):
            target = gain_buf.at[pl.ds(kv * n_tp, n_tp)]
            send(own_gains, target, GAINS, recv_sem.at[GAINS], k, 0)
        kv_gains = jnp.concatenate([gain_tp[t] for t in range(n_tp)], axis=1).astype(bf16)
        for i in range(4):
            loads["proj%d" % i].wait()
            based = jnp.dot(kv_gains, proj_v[i], preferred_element_type=f32)
            for h in range(heads):
                block = slice(h * HEAD, (h + 1) * HEAD)
                base_send[2 * i, h : h + 1, :] = based[0:1, block]
                base_send[2 * i + 1, h : h + 1, :] = based[2:3, block]
        for k in reversed(range(1, n_kv)):
            send(base_send.at[kv_of[k]], base_recv.at[kv], BASE, recv_sem.at[BASE], k, 0)
        base_recv[kv] = base_send[kv]

    gate = up = None
    for k in range(n_kv):
        source = kv_of[k]
        if k == n_kv // 2:
            send_bases()
        wait_for(tok_sem.at[source], tok_buf, n_tp if k else n_tp - 1)
        rows = jnp.concatenate([tok_buf[source * n_tp + t] for t in range(n_tp)], axis=1)
        cols = columns(source, group)
        if k == 0:
            loads["gate0"].wait()
            loads["up0"].wait()
        gate_part = dot_turned(rows, gate_v[0, :, cols])
        up_part = dot_turned(rows, up_v[0, :, cols])
        gate = gate_part if gate is None else gate + gate_part
        up = up_part if up is None else up + up_part
    reduce_scatter_start(hidden_of(gate, up), 0, RS_ONE, rs_recv_one)

    token_sum = jnp.sum(
        tree_sum([tok_buf[j].astype(f32) for j in range(n)]), axis=1, keepdims=True
    )
    centre = residual_scale * token_sum / width
    own_tokens = residual_scale * tok_buf[me].astype(f32) - centre

    wait_for(recv_sem.at[BASE], base_recv, n_kv - 1)
    base_all[kv] = tree_sum([base_recv[j] for j in range(n_kv)])
    for k in reversed(range(1, n_kv)):
        send(base_all.at[kv], base_all.at[kv], BASES, recv_sem.at[BASES], k, 0)
    shifted = own_tokens + 0.5 * reduce_scatter_end(RS_ONE, rs_recv_one)
    own_tp[tp] = (shifted * gains[0:1, :]).astype(bf16)
    for t in reversed(range(1, n_tp)):
        send(own_tp.at[tp], own_tp.at[tp], OWN_TP, recv_sem.at[OWN_TP], 0, t)
    for j in range(n_kv):
        turn_tp[tp, j] = shifted[j * seqs : (j + 1) * seqs, :]
    for t in reversed(range(1, n_tp)):
        send(turn_tp.at[tp], turn_tp.at[tp], TURN_TP, recv_sem.at[TURN_TP], 0, t)

    wait_for(recv_sem.at[OWN_TP], own_tp, n_tp - 1)
    block = jnp.concatenate([own_tp[t] for t in range(n_tp)], axis=1)
    wait_for(recv_sem.at[TURN_TP], turn_tp, n_tp - 1)
    own_turn = turn_recv.at[pl.ds(kv * n_tp, n_tp)]
    for k in reversed(range(1, n_kv)):
        send(turn_tp.at[:, kv_of[k]], own_turn, TURN, recv_sem.at[TURN], k, 0)
    for t in range(n_tp):
        turn_recv[kv * n_tp + t] = turn_tp[t, kv]
    turns = (1, 2, 0, 3)
    for i in turns:
        part = jnp.dot(block, proj_v[i], preferred_element_type=f32)
        for h in range(heads):
            for r in range(0, batch, 8):
                proj_f32[i, pl.ds(r * heads + h, 8, stride=heads), :] = part[
                    r : r + 8, h * HEAD : (h + 1) * HEAD
                ]
        proj_send[i] = proj_f32[i].reshape(proj_send.shape[1:]).astype(bf16)
        for k in reversed(range(1, n_kv)):
            send(proj_send.at[i, kv_of[k]], proj_recv.at[i, kv], PROJ, proj_sem.at[i], k, 0)
        proj_recv[i, kv] = proj_send[i, kv]

    wait_for(recv_sem.at[TURN], turn_recv, n - n_tp)

    def norm_stats(tiles):
        mean = total_of(tiles) / width
        centred = [tile - mean for tile in tiles]
        scale = lax.rsqrt(total_of([c * c for c in centred]) / width + norm_eps)
        return mean, scale, centred

    def normed_rows(stats, index):
        return [
            (
                tile * stats[1] * gain_buf[c * per : (c + 1) * per, index, :]
                + gain_buf[c * per : (c + 1) * per, 2 + index, :]
            ).astype(bf16)
            for c, tile in enumerate(stats[2])
        ]

    norm_one = [
        norm_stats([turn_recv[c * per : (c + 1) * per, s, :] for c in range(parts)])
        for s in range(seqs)
    ]
    wait_for(recv_sem.at[BASES], base_all, n_kv - 1)

    def projected(i):
        wait_for(proj_sem.at[i], proj_recv.at[i], n_kv - 1)
        total = tree_sum([proj_recv[i, j].astype(f32) for j in range(n_kv)])
        found = []
        for s in range(seqs):
            mean, scale, _ = norm_one[s]
            rows = total[s * heads : (s + 1) * heads] - mean * base_all[2 * i]
            rows = scale * rows + base_all[2 * i + 1]
            found.append(rows.astype(bf16).astype(f32))
        return found

    loads["low"].wait()
    low = low_v[...]
    forget_pre = projected(1)
    forget = [low + (1.0 - low) * jax.nn.sigmoid(p) for p in forget_pre]
    key_part = [(1.0 - low) * jax.nn.sigmoid(-p) for p in forget_pre]
    input_pre = projected(2)
    query = [jax.nn.silu(p) for p in projected(0)]
    fill = jnp.zeros((HEAD - 3 * seqs * heads, HEAD), f32)
    seen = [q * f for q, f in zip(query, forget)]
    turned = jnp.concatenate([*seen, *forget, *key_part, fill], axis=0).T

    def column(kind, s, h):
        first = (kind * seqs + s) * heads + h
        return turned[:, first : first + 1]

    loads["state"].wait()
    readouts = []
    for s in range(seqs):
        rows = [
            jnp.sum(column(0, s, h) * state_v[s, h], axis=0, keepdims=True) for h in range(heads)
        ]
        match = jnp.sum(query[s] * key_part[s], axis=1, keepdims=True)
        readout = jnp.concatenate(rows, axis=0) + match * input_pre[s]
        mean_square = jnp.mean(readout * readout, axis=1, keepdims=True)
        readouts.append(readout * lax.rsqrt(mean_square + head_eps))
    loads["head_gain"].wait()
    outgate = projected(3)
    for s in range(seqs):
        gated_buf[s * heads : (s + 1) * heads, :] = (
            readouts[s] * head_gain_v[...] * jax.nn.silu(outgate[s])
        )
    gated = jnp.concatenate(
        [gated_buf[pl.ds(h, seqs, stride=heads), :] for h in range(heads)], axis=1
    ).astype(bf16)
    loads["out"].wait()
    step = per * lane
    for c in range(parts):
        part = jnp.dot(gated, out_v[:, c * step : (c + 1) * step], preferred_element_type=f32)
        for j in range(per):
            head_f32[c, pl.ds(j, seqs, stride=per), :] = part[:, j * lane : (j + 1) * lane]
        head_buf[c, tp] = head_f32[c].astype(bf16)
        for t in reversed(range(1, n_tp)):
            send(head_buf.at[c, tp], head_buf.at[c, tp], HEADS_SUM, head_sem.at[c], 0, t)

    for s in range(seqs):
        for h in range(heads):
            new_v[s, h] = (
                column(1, s, h) * state_v[s, h] + column(2, s, h) * input_pre[s][h : h + 1, :]
            )

    wait_for(recv_sem.at[GAINS], gain_buf, n - n_tp)
    residual = [
        [residual_scale * tile.astype(f32) for tile in normed_rows(norm_one[s], 0)]
        for s in range(seqs)
    ]
    streams = [[] for _ in range(seqs)]
    for c in range(parts):
        wait_for(head_sem.at[c], head_buf.at[c], n_tp - 1)
        head_total = tree_sum([head_buf[c, t].astype(f32) for t in range(n_tp)])
        for s in range(seqs):
            mixed_rows = residual[s][c] + head_total[s * per : (s + 1) * per]
            streams[s].append(mixed_rows.astype(bf16).astype(f32))
    norm_two = [normed_rows(norm_stats(streams[s]), 1) for s in range(seqs)]
    for c in range(parts):
        ag_two[c, kv] = jnp.concatenate([norm_two[s][c] for s in range(seqs)], axis=0)
        for k in reversed(range(1, n_kv)):
            send(ag_two.at[c, kv], ag_two.at[c, kv], AG_TWO, ag_sem.at[c], k, 0)

    wait_for(send_sem.at[RS_ONE], rs_recv_one, n - 1)
    loads["gate1"].wait()
    loads["up1"].wait()
    gate = up = None
    for c in range(parts):
        wait_for(ag_sem.at[c], ag_two.at[c], n_kv - 1)
        ag_two_f32[c] = ag_two[c].astype(f32).reshape(ag_two_f32.shape[1:])
        tiles = []
        for j in range(per):
            pieces = [
                ag_two_f32[c, pl.ds(s * per + j, n_kv, stride=part_rows), :] for s in range(seqs)
            ]
            tiles.append(jnp.concatenate(pieces, axis=0).astype(bf16))
            normed_bf[c * per + j] = tiles[-1]
        rows = jnp.concatenate(tiles, axis=1)
        cols = slice(c * step, (c + 1) * step)
        gate_part = dot_turned(rows, gate_v[1, :, cols])
        up_part = dot_turned(rows, up_v[1, :, cols])
        gate = gate_part if gate is None else gate + gate_part
        up = up_part if up is None else up + up_part
    reduce_scatter_start(hidden_of(gate, up), 1, RS_THREE, rs_recv_three)
    own_rows = residual_scale * normed_bf[me].astype(f32)

    row_ids = lax.broadcasted_iota(jnp.int32, (batch, lane), 0)
    lane_ids = lax.broadcasted_iota(jnp.int32, (batch, lane), 1)
    stream = own_rows + 0.5 * reduce_scatter_end(RS_THREE, rs_recv_three)
    own_mean = jnp.sum(stream, axis=1, keepdims=True) / lane
    own_centred = stream - own_mean
    own_spread = jnp.sum(own_centred * own_centred, axis=1, keepdims=True)

    def to_lanes(values):
        return jnp.sum(jnp.where(row_ids == lane_ids, values, 0.0), axis=0, keepdims=True)

    spread_buf[me] = jnp.concatenate([to_lanes(own_mean), to_lanes(own_spread)], axis=0)
    for k, t in peers:
        send(spread_buf.at[me], spread_buf.at[me], SPREAD, recv_sem.at[SPREAD], k, t)

    for s in range(seqs):
        final_buf[pl.ds(s, n_kv, stride=seqs), :] = stream[s * n_kv : (s + 1) * n_kv, :]
    natural = final_buf[...]
    for kind in (TOK, RS_THREE):
        wait_for(send_sem.at[kind], tok_buf, n - 1)
    wait_for(send_sem.at[GAINS], gain_buf, n - n_tp)
    wait_for(send_sem.at[TURN_TP], turn_tp, n_tp - 1)
    wait_for(send_sem.at[GAIN_TP], gain_tp, n_tp - 1)
    wait_for(send_sem.at[TURN], turn_recv, n - n_tp)
    wait_for(send_sem.at[OWN_TP], own_tp, n_tp - 1)
    wait_for(send_sem.at[BASE], base_recv, n_kv - 1)
    wait_for(send_sem.at[BASES], base_all, n_kv - 1)
    for i in range(4):
        wait_for(send_sem.at[PROJ], proj_recv.at[i], n_kv - 1)
    for c in range(parts):
        wait_for(send_sem.at[HEADS_SUM], head_buf.at[c], n_tp - 1)
        wait_for(send_sem.at[AG_TWO], ag_two.at[c], n_kv - 1)

    wait_for(recv_sem.at[SPREAD], spread_buf, n - 1)
    means = spread_buf[:, 0, :]
    mean_row = jnp.sum(means, axis=0, keepdims=True) / n
    apart = means - mean_row
    square_row = jnp.sum(spread_buf[:, 1, :] + lane * (apart * apart), axis=0, keepdims=True)
    scale_row = lax.rsqrt(square_row / width + norm_eps)
    place = lax.rem(row_ids, seqs) * n_kv + lax.div(row_ids, seqs)

    def to_rows(values):
        return jnp.sum(jnp.where(place == lane_ids, values, 0.0), axis=1, keepdims=True)

    mixed = (natural - to_rows(mean_row)) * to_rows(scale_row) * gains[4:5, :] + gains[5:6, :]
    mixed_ref[...] = mixed.astype(bf16)
    wait_for(send_sem.at[SPREAD], spread_buf, n - 1)


def store_kernel(mixed_v, new_v, mixed_out, state_out, sem):
    copies = [
        pltpu.make_async_copy(new_v, state_out, sem.at[0]),
        pltpu.make_async_copy(mixed_v, mixed_out, sem.at[1]),
    ]
    for copy in copies:
        copy.start()
    for copy in copies:
        copy.wait()


def fused(n_kv, n_tp, *args):
    (
        tokens,
        gate_weights,
        up_weights,
        down_weights,
        norm_gain,
        norm_bias,
        query_weight,
        forget_weight,
        input_weight,
        outgate_weight,
        lower_bound,
        head_gain,
        out_weight,
        state,
    ) = args
    batch, lane = tokens.shape
    n = n_kv * n_tp
    seqs, heads = state.shape[:2]
    gate_weights = jnp.swapaxes(gate_weights, 1, 2)
    up_weights = jnp.swapaxes(up_weights, 1, 2)
    bf16, f32 = jnp.bfloat16, jnp.float32
    per = 8
    parts, part_rows = n // per, per * seqs
    seq_rows = seqs * heads
    scratch = [
        pltpu.VMEM(gate_weights.shape, bf16),
        pltpu.VMEM(up_weights.shape, bf16),
        pltpu.VMEM(down_weights.shape, bf16),
        pltpu.VMEM((4, *query_weight.shape), bf16),
        pltpu.VMEM(out_weight.shape, bf16),
        pltpu.VMEM(state.shape, f32),
        pltpu.VMEM(norm_gain.shape, bf16),
        pltpu.VMEM(norm_bias.shape, bf16),
        pltpu.VMEM((heads, HEAD), f32),
        pltpu.VMEM((heads, HEAD), f32),
        pltpu.VMEM((n, batch, lane), bf16),
        pltpu.VMEM((n_tp, 8, lane), f32),
        pltpu.VMEM((n, 4, lane), f32),
        pltpu.VMEM((n, batch, lane), bf16),
        pltpu.VMEM((n, batch, lane), bf16),
        pltpu.VMEM((n, batch, lane), bf16),
        pltpu.VMEM((n_tp, n_kv, seqs, lane), f32),
        pltpu.VMEM((n, seqs, lane), f32),
        pltpu.VMEM((n_tp, batch, lane), bf16),
        pltpu.VMEM((n_kv, heads, HEAD), f32),
        pltpu.VMEM((n_kv, heads, HEAD), f32),
        pltpu.VMEM((n_kv, heads, HEAD), f32),
        pltpu.VMEM((4, batch * heads, HEAD), f32),
        pltpu.VMEM((4, n_kv, seq_rows, HEAD), bf16),
        pltpu.VMEM((4, n_kv, seq_rows, HEAD), bf16),
        pltpu.VMEM((seq_rows, HEAD), f32),
        pltpu.VMEM((parts, part_rows, lane), f32),
        pltpu.VMEM((parts, n_tp, part_rows, lane), bf16),
        pltpu.VMEM((parts, n_kv, part_rows, lane), bf16),
        pltpu.VMEM((parts, n_kv * part_rows, lane), f32),
        pltpu.VMEM((n, batch, lane), bf16),
        pltpu.VMEM((n, 2, lane), f32),
        pltpu.VMEM((batch, lane), f32),
        pltpu.SemaphoreType.DMA((len(KINDS) + 4,)),
        pltpu.SemaphoreType.DMA((len(KINDS),)),
        pltpu.SemaphoreType.DMA((n_kv,)),
        pltpu.SemaphoreType.DMA((4,)),
        pltpu.SemaphoreType.DMA((parts,)),
        pltpu.SemaphoreType.DMA((parts,)),
        pltpu.SemaphoreType.DMA((17,)),
    ]
    vmem = pl.BlockSpec(memory_space=pltpu.VMEM)
    hbm = pl.BlockSpec(memory_space=pl.ANY)
    held = pl.pallas_call(
        functools.partial(layer_kernel, n_kv, n_tp),
        out_shape=(pltpu.VMEM(tokens.shape, bf16), pltpu.VMEM(state.shape, f32)),
        in_specs=[hbm] * 14,
        out_specs=(vmem, vmem),
        scratch_shapes=scratch,
        compiler_params=pltpu.CompilerParams(
            collective_id=0, has_side_effects=True, vmem_limit_bytes=44 * 1024 * 1024
        ),
        name="layer",
    )(*[pltpu.with_memory_space_constraint(operand, pltpu.HBM) for operand in (
        tokens,
        norm_gain,
        norm_bias,
        lower_bound.reshape(heads, HEAD),
        head_gain.reshape(heads, HEAD),
        gate_weights,
        up_weights,
        down_weights,
        query_weight,
        forget_weight,
        input_weight,
        outgate_weight,
        out_weight,
        state,
    )])
    return pl.pallas_call(
        store_kernel,
        out_shape=(
            jax.ShapeDtypeStruct(tokens.shape, bf16),
            jax.ShapeDtypeStruct(state.shape, f32),
        ),
        in_specs=[vmem, vmem],
        out_specs=(hbm, hbm),
        scratch_shapes=[pltpu.SemaphoreType.DMA((2,))],
        compiler_params=pltpu.CompilerParams(vmem_limit_bytes=4 * 1024 * 1024),
        name="store",
    )(*held)


def power_of_two(count):
    return count & (count - 1) == 0


def dispatch(n_kv, n_tp, *args):
    tokens, state = args[0], args[13]
    batch, lane = tokens.shape
    seqs, heads = state.shape[:2]
    fits = lane == HEAD and batch == 16 and heads == 8 and seqs == 2 and n_kv == 8
    if fits and power_of_two(n_tp) and n_kv * n_tp % 8 == 0:
        return fused(n_kv, n_tp, *args)
    return local(*args)


def solution(mesh):
    n_kv, n_tp = mesh.shape["kv"], mesh.shape["tp"]
    return jax.shard_map(
        functools.partial(dispatch, n_kv, n_tp),
        mesh=mesh,
        in_specs=(
            P(None, ("kv", "tp")),
            P(None, None, ("kv", "tp")),
            P(None, None, ("kv", "tp")),
            P(None, ("kv", "tp"), None),
            P(None, ("kv", "tp")),
            P(None, ("kv", "tp")),
            P("kv", "tp"),
            P("kv", "tp"),
            P("kv", "tp"),
            P("kv", "tp"),
            P("tp"),
            P("tp"),
            P("tp", None),
            P("kv", "tp", None, None),
        ),
        out_specs=(P(None, ("kv", "tp")), P("kv", "tp", None, None)),
        check_vma=False,
    )
```

```python
import functools

import jax
import jax.numpy as jnp
from jax import lax
from jax.experimental import pallas as pl
from jax.experimental.pallas import tpu as pltpu
from jax.sharding import PartitionSpec as P

MESH = pl.DeviceIdType.MESH

HEAD = 128


residual_scale = 8.0**0.25
norm_eps = 1e-05
head_eps = 1e-06


def whole_norm(stream, gain_row, bias_row):
    row_mean = jnp.mean(stream, axis=-1, keepdims=True)
    centred = stream - row_mean
    spread = jnp.mean(centred * centred, axis=-1, keepdims=True)
    return centred * lax.rsqrt(spread + norm_eps) * gain_row.astype(jnp.float32) + bias_row.astype(
        jnp.float32
    )


def ffn_partial(whole_rows, gate_w, up_w, down_w):
    gate_proj = jnp.dot(whole_rows, gate_w, preferred_element_type=jnp.float32)
    up_proj = jnp.dot(whole_rows, up_w, preferred_element_type=jnp.float32)
    hidden = (jax.nn.silu(gate_proj) * up_proj).astype(jnp.bfloat16)
    return jnp.dot(hidden, down_w, preferred_element_type=jnp.float32)


def local(
    tokens,
    gate_weights,
    up_weights,
    down_weights,
    norm_gain,
    norm_bias,
    query_weight,
    forget_weight,
    input_weight,
    outgate_weight,
    lower_bound,
    head_gain,
    out_weight,
    state,
):
    own_cols = tokens.shape[1]
    col_offset = lax.axis_index(("kv", "tp")) * own_cols
    whole_tokens, whole_gain, whole_bias = (
        lax.all_gather(tokens, ("kv", "tp"), axis=1, tiled=True),
        lax.all_gather(norm_gain, ("kv", "tp"), axis=1, tiled=True),
        lax.all_gather(norm_bias, ("kv", "tp"), axis=1, tiled=True),
    )

    def finish(partial_value, residual_whole, index, want_whole):
        total = lax.psum(partial_value, ("kv", "tp"))
        stream = residual_scale * residual_whole + 0.5 * total
        normed = whole_norm(stream, whole_gain[index], whole_bias[index]).astype(jnp.bfloat16)
        if want_whole:
            return normed
        return lax.dynamic_slice_in_dim(normed, col_offset, own_cols, 1)

    partial_one = ffn_partial(whole_tokens, gate_weights[0], up_weights[0], down_weights[0])
    normed_one = finish(partial_one, whole_tokens.astype(jnp.float32), 0, True)
    seq_count = state.shape[0]
    head_count = state.shape[1]
    head_cols = query_weight.shape[1]
    weight_rows = query_weight.shape[0]
    seq_offset = lax.axis_index("kv") * seq_count
    block_rows = lax.dynamic_slice_in_dim(
        normed_one, lax.axis_index("kv") * weight_rows, weight_rows, 1
    )
    weights = (query_weight, forget_weight, input_weight, outgate_weight)
    projected = lax.psum_scatter(
        jnp.concatenate(
            [jnp.dot(block_rows, weight, preferred_element_type=jnp.float32) for weight in weights],
            axis=1,
        ).astype(jnp.bfloat16),
        "kv",
        scatter_dimension=0,
        tiled=True,
    )
    query_pre = projected[:, :head_cols].astype(jnp.float32).reshape(seq_count, head_count, HEAD)
    forget_pre = (
        projected[:, head_cols : 2 * head_cols]
        .astype(jnp.float32)
        .reshape(seq_count, head_count, HEAD)
    )
    input_pre = (
        projected[:, 2 * head_cols : 3 * head_cols]
        .astype(jnp.float32)
        .reshape(seq_count, head_count, HEAD)
    )
    outgate_pre = projected[:, 3 * head_cols :].astype(jnp.float32)
    low_bound = lower_bound.reshape(head_count, HEAD)
    forget = low_bound + (1.0 - low_bound) * jax.nn.sigmoid(forget_pre)
    key_part = (1.0 - low_bound) * jax.nn.sigmoid(-forget_pre)
    updated = forget[..., None] * state + key_part[..., None] * input_pre[:, :, None, :]
    readout = jnp.einsum(
        "shd,shde->she", jax.nn.silu(query_pre), updated, precision=lax.Precision.HIGHEST
    )
    readout = readout * lax.rsqrt(jnp.mean(readout * readout, axis=-1, keepdims=True) + head_eps)
    gated_out = (
        readout.reshape(seq_count, head_cols) * head_gain * jax.nn.silu(outgate_pre)
    ).astype(jnp.bfloat16)
    mixer_part = jnp.dot(gated_out, out_weight, preferred_element_type=jnp.float32)
    head_sum = lax.psum_scatter(
        mixer_part.astype(jnp.bfloat16), "tp", scatter_dimension=1, tiled=True
    ).astype(jnp.float32)
    piece_cols = head_sum.shape[1]
    own_normed = lax.dynamic_slice_in_dim(normed_one, seq_offset, seq_count, 0)
    own_normed = lax.dynamic_slice_in_dim(
        own_normed, lax.axis_index("tp") * piece_cols, piece_cols, 1
    )
    stream_own = (residual_scale * own_normed.astype(jnp.float32) + head_sum).astype(jnp.bfloat16)
    seq_rows = lax.all_gather(stream_own, "tp", axis=1, tiled=True)
    stream_two = lax.all_gather(seq_rows, "kv", axis=0, tiled=True)
    normed_two = whole_norm(stream_two.astype(jnp.float32), whole_gain[1], whole_bias[1]).astype(
        jnp.bfloat16
    )
    partial_two = ffn_partial(normed_two, gate_weights[1], up_weights[1], down_weights[1])
    mixed = finish(partial_two, normed_two.astype(jnp.float32), 2, False)
    return (mixed, updated)


KINDS = ("gain_tp", "gains", "rs_one", "turn", "turn_tp", "own_tp", "base", "bases", "stat_two", "rs_three", "spread")


def tree_sum(terms):
    while len(terms) > 1:
        rest = [terms[-1]] if len(terms) % 2 else []
        terms = [a + b for a, b in zip(terms[::2], terms[1::2])] + rest
    return terms[0]


def total_of(tiles):
    rows = jnp.sum(tree_sum(tiles), axis=0, keepdims=True)
    return jnp.sum(rows, axis=1, keepdims=True)


def dot_turned(rows, weights):
    return lax.dot_general(
        rows, weights, (((1,), (1,)), ((), ())), preferred_element_type=jnp.float32
    )


def flipped(value, count, mask):
    out, bit = value, 1
    while bit < count:
        if mask & bit:
            out = out + bit - 2 * bit * lax.rem(lax.div(value, bit), 2)
        bit *= 2
    return out


def layer_kernel(
    n_kv,
    n_tp,
    tokens_hbm,
    gain_hbm,
    bias_hbm,
    low_hbm,
    head_gain_hbm,
    gate_hbm,
    up_hbm,
    down_hbm,
    query_hbm,
    forget_hbm,
    input_hbm,
    outgate_hbm,
    out_hbm,
    state_hbm,
    mixed_ref,
    new_v,
    gate_v,
    up_v,
    gate_t,
    up_t,
    down_v,
    proj_v,
    out_v,
    state_v,
    gain_v,
    bias_v,
    low_v,
    head_gain_v,
    tok_buf,
    gain_tp,
    gain_buf,
    rs_send,
    rs_recv_one,
    rs_recv_three,
    turn_tp,
    turn_recv,
    own_tp,
    base_send,
    base_recv,
    base_all,
    proj_f32,
    proj_send,
    proj_recv,
    gated_buf,
    head_f32,
    head_buf,
    ag_two,
    ag_two_f32,
    stat_two,
    normed_bf,
    spread_buf,
    final_buf,
    send_sem,
    recv_sem,
    tok_sem,
    proj_sem,
    head_sem,
    ag_sem,
    load_sem,
):
    n = n_kv * n_tp
    batch, lane = tok_buf.shape[1:]
    width = n * lane
    seqs, heads = state_v.shape[0], state_v.shape[1]
    part_rows = ag_two.shape[2]
    per = part_rows // seqs
    parts = n // per
    group = n_tp * lane
    bf16, f32 = jnp.bfloat16, jnp.float32
    kv, tp = lax.axis_index("kv"), lax.axis_index("tp")
    me = kv * n_tp + tp
    kv_of = [flipped(kv, n_kv, m) for m in range(n_kv)]
    tp_of = [flipped(tp, n_tp, m) for m in range(n_tp)]
    peers = [(k, t) for k in reversed(range(n_kv)) for t in reversed(range(n_tp)) if k or t]

    barrier = pltpu.get_barrier_semaphore()
    for k, t in peers:
        pl.semaphore_signal(
            barrier, inc=1, device_id=(kv_of[k], tp_of[t]), device_id_type=MESH
        )

    proj_hbm = (query_hbm, forget_hbm, input_hbm, outgate_hbm)
    loads = {}
    order = [("tokens", tokens_hbm, tok_buf.at[me])]
    order += [("gain", gain_hbm, gain_v), ("bias", bias_hbm, bias_v)]
    order += [("gate0", gate_hbm.at[0], gate_v.at[0]), ("up0", up_hbm.at[0], up_v.at[0])]
    order += [("down0", down_hbm.at[0], down_v.at[0])]
    order += [("proj%d" % i, proj_hbm[i], proj_v.at[i]) for i in range(4)]
    order += [("low", low_hbm, low_v), ("head_gain", head_gain_hbm, head_gain_v)]
    order += [("state", state_hbm, state_v), ("out", out_hbm, out_v)]
    order += [("gate1", gate_hbm.at[1], gate_v.at[1]), ("up1", up_hbm.at[1], up_v.at[1])]
    order += [("down1", down_hbm.at[1], down_v.at[1])]
    for i, (name, source, target) in enumerate(order):
        loads[name] = pltpu.make_async_copy(source, target, load_sem.at[i])
        if i < 10:
            loads[name].start()

    def send(src, dst, kind, recv, k, t):
        pltpu.make_async_remote_copy(
            src_ref=src,
            dst_ref=dst,
            send_sem=send_sem.at[kind],
            recv_sem=recv,
            device_id=(kv_of[k], tp_of[t]),
            device_id_type=MESH,
        ).start()

    def wait_for(sem, ref, count):
        part = ref.at[pl.ds(0, count)]
        pltpu.make_async_copy(part, part, sem).wait()

    GAIN_TP, GAINS, RS_ONE, TURN, TURN_TP, OWN_TP, BASE, BASES, STAT_TWO, RS_THREE, SPREAD = range(len(KINDS))
    TOK, PROJ, HEADS_SUM, AG_TWO = range(len(KINDS), len(KINDS) + 4)

    loads["gain"].wait()
    loads["bias"].wait()
    pad = jnp.zeros((2, lane), f32)
    gains, biases = gain_v[...].astype(f32), bias_v[...].astype(f32)
    gains = jnp.concatenate([gains[0:2], biases[0:2], gains[2:3], biases[2:3], pad], axis=0)
    gain_tp[tp] = gains
    loads["tokens"].wait()
    pl.semaphore_wait(barrier, n - 1)
    for k, t in peers:
        send(tok_buf.at[me], tok_buf.at[me], TOK, tok_sem.at[kv], k, t)
    for t in reversed(range(1, n_tp)):
        send(gain_tp.at[tp], gain_tp.at[tp], GAIN_TP, recv_sem.at[GAIN_TP], 0, t)

    for name in [entry[0] for entry in order[10:]]:
        loads[name].start()

    def columns(index, size):
        return pl.ds(pl.multiple_of(index * size, size), size)

    def hidden_of(gate, up):
        return (jax.nn.silu(gate) * up).astype(bf16)

    def reduce_scatter_start(hidden, layer, kind, recv):
        loads["down%d" % layer].wait()
        for k in reversed(range(n_kv)):
            target = kv_of[k]
            part = jnp.dot(
                hidden, down_v[layer, :, columns(target, group)], preferred_element_type=f32
            ).astype(bf16)
            for t in range(n_tp):
                rs_send[target * n_tp + t] = part[:, t * lane : (t + 1) * lane]
            for t in reversed(range(n_tp)):
                if k or t:
                    index = target * n_tp + tp_of[t]
                    send(rs_send.at[index], recv.at[me], kind, recv_sem.at[kind], k, t)
        recv[me] = rs_send[me]

    def reduce_scatter_end(kind, recv):
        wait_for(recv_sem.at[kind], recv, n - 1)
        return tree_sum([recv[j].astype(f32) for j in range(n)])

    def turn_weights(layer):
        loads["gate%d" % layer].wait()
        loads["up%d" % layer].wait()
        for source, target in ((gate_v, gate_t), (up_v, up_t)):

            @pl.loop(0, width // (2 * lane))
            def _(i):
                rows = columns(i, 2 * lane)
                target[layer, rows, :] = source[layer, :, rows].T

    def send_bases():
        wait_for(recv_sem.at[GAIN_TP], gain_tp, n_tp - 1)
        for t in range(n_tp):
            gain_buf[kv * n_tp + t] = gain_tp[t, 0:4]
        own_gains = gain_tp.at[:, pl.ds(0, 4)]
        for k in reversed(range(1, n_kv)):
            target = gain_buf.at[pl.ds(kv * n_tp, n_tp)]
            send(own_gains, target, GAINS, recv_sem.at[GAINS], k, 0)
        kv_gains = jnp.concatenate([gain_tp[t] for t in range(n_tp)], axis=1).astype(bf16)
        for i in range(4):
            loads["proj%d" % i].wait()
            based = jnp.dot(kv_gains, proj_v[i], preferred_element_type=f32)
            for h in range(heads):
                block = slice(h * HEAD, (h + 1) * HEAD)
                base_send[2 * i, h : h + 1, :] = based[0:1, block]
                base_send[2 * i + 1, h : h + 1, :] = based[2:3, block]
        for k in reversed(range(1, n_kv)):
            send(base_send.at[kv_of[k]], base_recv.at[kv], BASE, recv_sem.at[BASE], k, 0)
        base_recv[kv] = base_send[kv]

    turn_weights(0)
    gate = up = None
    for k in range(n_kv):
        source = kv_of[k]
        wait_for(tok_sem.at[source], tok_buf, n_tp if k else n_tp - 1)
        rows = jnp.concatenate([tok_buf[source * n_tp + t] for t in range(n_tp)], axis=1)
        cols = columns(source, group)
        gate_part = jnp.dot(rows, gate_t[0, cols, :], preferred_element_type=f32)
        up_part = jnp.dot(rows, up_t[0, cols, :], preferred_element_type=f32)
        gate = gate_part if gate is None else gate + gate_part
        up = up_part if up is None else up + up_part
    reduce_scatter_start(hidden_of(gate, up), 0, RS_ONE, rs_recv_one)

    send_bases()
    turn_weights(1)
    token_sum = jnp.sum(
        tree_sum([tok_buf[j].astype(f32) for j in range(n)]), axis=1, keepdims=True
    )
    centre = residual_scale * token_sum / width
    own_tokens = residual_scale * tok_buf[me].astype(f32) - centre

    shifted = own_tokens + 0.5 * reduce_scatter_end(RS_ONE, rs_recv_one)
    own_tp[tp] = (shifted * gains[0:1, :]).astype(bf16)
    for t in reversed(range(1, n_tp)):
        send(own_tp.at[tp], own_tp.at[tp], OWN_TP, recv_sem.at[OWN_TP], 0, t)
    for j in range(n_kv):
        turn_tp[tp, j] = shifted[j * seqs : (j + 1) * seqs, :]
    for t in reversed(range(1, n_tp)):
        send(turn_tp.at[tp], turn_tp.at[tp], TURN_TP, recv_sem.at[TURN_TP], 0, t)

    wait_for(recv_sem.at[BASE], base_recv, n_kv - 1)
    base_all[kv] = tree_sum([base_recv[j] for j in range(n_kv)])
    for k in reversed(range(1, n_kv)):
        send(base_all.at[kv], base_all.at[kv], BASES, recv_sem.at[BASES], k, 0)
    wait_for(recv_sem.at[OWN_TP], own_tp, n_tp - 1)
    block = jnp.concatenate([own_tp[t] for t in range(n_tp)], axis=1)
    wait_for(recv_sem.at[TURN_TP], turn_tp, n_tp - 1)
    own_turn = turn_recv.at[pl.ds(kv * n_tp, n_tp)]
    for k in reversed(range(1, n_kv)):
        send(turn_tp.at[:, kv_of[k]], own_turn, TURN, recv_sem.at[TURN], k, 0)
    for t in range(n_tp):
        turn_recv[kv * n_tp + t] = turn_tp[t, kv]
    turns = (1, 2, 0, 3)
    for i in turns:
        part = jnp.dot(block, proj_v[i], preferred_element_type=f32)
        for h in range(heads):
            for r in range(0, batch, 8):
                proj_f32[i, pl.ds(r * heads + h, 8, stride=heads), :] = part[
                    r : r + 8, h * HEAD : (h + 1) * HEAD
                ]
        proj_send[i] = proj_f32[i].reshape(proj_send.shape[1:]).astype(bf16)
        for k in reversed(range(1, n_kv)):
            send(proj_send.at[i, kv_of[k]], proj_recv.at[i, kv], PROJ, proj_sem.at[i], k, 0)
        proj_recv[i, kv] = proj_send[i, kv]

    wait_for(recv_sem.at[GAINS], gain_buf, n - n_tp)
    all_gains = jnp.concatenate([gain_buf[j] for j in range(n)], axis=1).astype(bf16)
    gate_fixed = jnp.dot(all_gains, gate_t[1], preferred_element_type=f32)
    up_fixed = jnp.dot(all_gains, up_t[1], preferred_element_type=f32)
    wait_for(recv_sem.at[TURN], turn_recv, n - n_tp)

    def norm_stats(tiles):
        mean = total_of(tiles) / width
        centred = [tile - mean for tile in tiles]
        scale = lax.rsqrt(total_of([c * c for c in centred]) / width + norm_eps)
        return mean, scale, centred

    def normed_rows(stats, index):
        return [
            (
                tile * stats[1] * gain_buf[c * per : (c + 1) * per, index, :]
                + gain_buf[c * per : (c + 1) * per, 2 + index, :]
            ).astype(bf16)
            for c, tile in enumerate(stats[2])
        ]

    norm_one = [
        norm_stats([turn_recv[c * per : (c + 1) * per, s, :] for c in range(parts)])
        for s in range(seqs)
    ]
    wait_for(recv_sem.at[BASES], base_all, n_kv - 1)

    def projected(i):
        wait_for(proj_sem.at[i], proj_recv.at[i], n_kv - 1)
        total = tree_sum([proj_recv[i, j].astype(f32) for j in range(n_kv)])
        found = []
        for s in range(seqs):
            mean, scale, _ = norm_one[s]
            rows = total[s * heads : (s + 1) * heads] - mean * base_all[2 * i]
            rows = scale * rows + base_all[2 * i + 1]
            found.append(rows.astype(bf16).astype(f32))
        return found

    loads["low"].wait()
    low = low_v[...]
    forget_pre = projected(1)
    forget = [low + (1.0 - low) * jax.nn.sigmoid(p) for p in forget_pre]
    key_part = [(1.0 - low) * jax.nn.sigmoid(-p) for p in forget_pre]
    input_pre = projected(2)
    query = [jax.nn.silu(p) for p in projected(0)]
    fill = jnp.zeros((HEAD - 3 * seqs * heads, HEAD), f32)
    seen = [q * f for q, f in zip(query, forget)]
    turned = jnp.concatenate([*seen, *forget, *key_part, fill], axis=0).T

    def column(kind, s, h):
        first = (kind * seqs + s) * heads + h
        return turned[:, first : first + 1]

    loads["state"].wait()
    readouts = []
    for s in range(seqs):
        rows = [
            jnp.sum(column(0, s, h) * state_v[s, h], axis=0, keepdims=True) for h in range(heads)
        ]
        match = jnp.sum(query[s] * key_part[s], axis=1, keepdims=True)
        readout = jnp.concatenate(rows, axis=0) + match * input_pre[s]
        mean_square = jnp.mean(readout * readout, axis=1, keepdims=True)
        readouts.append(readout * lax.rsqrt(mean_square + head_eps))
    loads["head_gain"].wait()
    outgate = projected(3)
    for s in range(seqs):
        gated_buf[s * heads : (s + 1) * heads, :] = (
            readouts[s] * head_gain_v[...] * jax.nn.silu(outgate[s])
        )
    gated = jnp.concatenate(
        [gated_buf[pl.ds(h, seqs, stride=heads), :] for h in range(heads)], axis=1
    ).astype(bf16)
    loads["out"].wait()
    step = per * lane
    for c in range(parts):
        part = jnp.dot(gated, out_v[:, c * step : (c + 1) * step], preferred_element_type=f32)
        for j in range(per):
            head_f32[c, pl.ds(j, seqs, stride=per), :] = part[:, j * lane : (j + 1) * lane]
        head_buf[c, tp] = head_f32[c].astype(bf16)
        for t in reversed(range(1, n_tp)):
            send(head_buf.at[c, tp], head_buf.at[c, tp], HEADS_SUM, head_sem.at[c], 0, t)

    for s in range(seqs):
        for h in range(heads):
            new_v[s, h] = (
                column(1, s, h) * state_v[s, h] + column(2, s, h) * input_pre[s][h : h + 1, :]
            )

    residual = [
        [residual_scale * tile.astype(f32) for tile in normed_rows(norm_one[s], 0)]
        for s in range(seqs)
    ]
    middle = [total_of(residual[s]) / width for s in range(seqs)]
    streams = [[] for _ in range(seqs)]
    for c in range(parts):
        wait_for(head_sem.at[c], head_buf.at[c], n_tp - 1)
        head_total = tree_sum([head_buf[c, t].astype(f32) for t in range(n_tp)])
        for s in range(seqs):
            mixed_rows = residual[s][c] + head_total[s * per : (s + 1) * per]
            streams[s].append(mixed_rows.astype(bf16).astype(f32) - middle[s])
        gain_rows = gain_buf[c * per : (c + 1) * per, 1, :]
        ag_two[c, kv] = jnp.concatenate(
            [streams[s][c] * gain_rows for s in range(seqs)], axis=0
        ).astype(bf16)
        for k in reversed(range(1, n_kv)):
            send(ag_two.at[c, kv], ag_two.at[c, kv], AG_TWO, ag_sem.at[c], k, 0)
    stats = [norm_stats(streams[s]) for s in range(seqs)]
    for i in range(2):
        for s in range(seqs):
            row = jnp.broadcast_to(stats[s][i], (1, lane))
            stat_two[kv, i * seqs + s : i * seqs + s + 1, :] = row
    for k in reversed(range(1, n_kv)):
        send(stat_two.at[kv], stat_two.at[kv], STAT_TWO, recv_sem.at[STAT_TWO], k, 0)

    wait_for(send_sem.at[RS_ONE], rs_recv_one, n - 1)
    gate = up = None
    for c in range(parts):
        wait_for(ag_sem.at[c], ag_two.at[c], n_kv - 1)
        ag_two_f32[c] = ag_two[c].astype(f32).reshape(ag_two_f32.shape[1:])
        tiles = []
        for j in range(per):
            pieces = [
                ag_two_f32[c, pl.ds(s * per + j, n_kv, stride=part_rows), :] for s in range(seqs)
            ]
            tiles.append(jnp.concatenate(pieces, axis=0).astype(bf16))
            normed_bf[c * per + j] = tiles[-1]
        rows = jnp.concatenate(tiles, axis=1)
        cols = slice(c * step, (c + 1) * step)
        gate_part = jnp.dot(rows, gate_t[1, cols, :], preferred_element_type=f32)
        up_part = jnp.dot(rows, up_t[1, cols, :], preferred_element_type=f32)
        gate = gate_part if gate is None else gate + gate_part
        up = up_part if up is None else up + up_part
    wait_for(recv_sem.at[STAT_TWO], stat_two, n_kv - 1)
    mean_two, scale_two = [
        jnp.concatenate([stat_two[:, i * seqs + s, :] for s in range(seqs)], axis=0)[:, 0:1]
        for i in range(2)
    ]
    gate = scale_two * (gate - mean_two * gate_fixed[1:2]) + gate_fixed[3:4]
    up = scale_two * (up - mean_two * up_fixed[1:2]) + up_fixed[3:4]
    reduce_scatter_start(hidden_of(gate, up), 1, RS_THREE, rs_recv_three)
    own_rows = scale_two * (normed_bf[me].astype(f32) - mean_two * gains[1:2]) + gains[3:4]
    own_rows = residual_scale * own_rows

    row_ids = lax.broadcasted_iota(jnp.int32, (batch, lane), 0)
    lane_ids = lax.broadcasted_iota(jnp.int32, (batch, lane), 1)
    stream = own_rows + 0.5 * reduce_scatter_end(RS_THREE, rs_recv_three)
    own_mean = jnp.sum(stream, axis=1, keepdims=True) / lane
    own_centred = stream - own_mean
    own_spread = jnp.sum(own_centred * own_centred, axis=1, keepdims=True)

    def to_lanes(values):
        return jnp.sum(jnp.where(row_ids == lane_ids, values, 0.0), axis=0, keepdims=True)

    spread_buf[me] = jnp.concatenate([to_lanes(own_mean), to_lanes(own_spread)], axis=0)
    for k, t in peers:
        send(spread_buf.at[me], spread_buf.at[me], SPREAD, recv_sem.at[SPREAD], k, t)

    for s in range(seqs):
        final_buf[pl.ds(s, n_kv, stride=seqs), :] = stream[s * n_kv : (s + 1) * n_kv, :]
    natural = final_buf[...]
    for kind in (TOK, RS_THREE):
        wait_for(send_sem.at[kind], tok_buf, n - 1)
    wait_for(send_sem.at[GAINS], gain_buf, n - n_tp)
    wait_for(send_sem.at[TURN_TP], turn_tp, n_tp - 1)
    wait_for(send_sem.at[GAIN_TP], gain_tp, n_tp - 1)
    wait_for(send_sem.at[TURN], turn_recv, n - n_tp)
    wait_for(send_sem.at[OWN_TP], own_tp, n_tp - 1)
    wait_for(send_sem.at[BASE], base_recv, n_kv - 1)
    wait_for(send_sem.at[BASES], base_all, n_kv - 1)
    for i in range(4):
        wait_for(send_sem.at[PROJ], proj_recv.at[i], n_kv - 1)
    wait_for(send_sem.at[STAT_TWO], stat_two, n_kv - 1)
    for c in range(parts):
        wait_for(send_sem.at[HEADS_SUM], head_buf.at[c], n_tp - 1)
        wait_for(send_sem.at[AG_TWO], ag_two.at[c], n_kv - 1)

    wait_for(recv_sem.at[SPREAD], spread_buf, n - 1)
    means = spread_buf[:, 0, :]
    mean_row = jnp.sum(means, axis=0, keepdims=True) / n
    apart = means - mean_row
    square_row = jnp.sum(spread_buf[:, 1, :] + lane * (apart * apart), axis=0, keepdims=True)
    scale_row = lax.rsqrt(square_row / width + norm_eps)
    place = lax.rem(row_ids, seqs) * n_kv + lax.div(row_ids, seqs)

    def to_rows(values):
        return jnp.sum(jnp.where(place == lane_ids, values, 0.0), axis=1, keepdims=True)

    mixed = (natural - to_rows(mean_row)) * to_rows(scale_row) * gains[4:5, :] + gains[5:6, :]
    mixed_ref[...] = mixed.astype(bf16)
    wait_for(send_sem.at[SPREAD], spread_buf, n - 1)


def store_kernel(mixed_v, new_v, mixed_out, state_out, sem):
    copies = [
        pltpu.make_async_copy(new_v, state_out, sem.at[0]),
        pltpu.make_async_copy(mixed_v, mixed_out, sem.at[1]),
    ]
    for copy in copies:
        copy.start()
    for copy in copies:
        copy.wait()


def fused(n_kv, n_tp, *args):
    (
        tokens,
        gate_weights,
        up_weights,
        down_weights,
        norm_gain,
        norm_bias,
        query_weight,
        forget_weight,
        input_weight,
        outgate_weight,
        lower_bound,
        head_gain,
        out_weight,
        state,
    ) = args
    batch, lane = tokens.shape
    n = n_kv * n_tp
    seqs, heads = state.shape[:2]
    gate_weights = jnp.swapaxes(gate_weights, 1, 2)
    up_weights = jnp.swapaxes(up_weights, 1, 2)
    bf16, f32 = jnp.bfloat16, jnp.float32
    per = 8
    parts, part_rows = n // per, per * seqs
    seq_rows = seqs * heads
    scratch = [
        pltpu.VMEM(gate_weights.shape, bf16),
        pltpu.VMEM(up_weights.shape, bf16),
        pltpu.VMEM((2, n * lane, gate_weights.shape[1]), bf16),
        pltpu.VMEM((2, n * lane, gate_weights.shape[1]), bf16),
        pltpu.VMEM(down_weights.shape, bf16),
        pltpu.VMEM((4, *query_weight.shape), bf16),
        pltpu.VMEM(out_weight.shape, bf16),
        pltpu.VMEM(state.shape, f32),
        pltpu.VMEM(norm_gain.shape, bf16),
        pltpu.VMEM(norm_bias.shape, bf16),
        pltpu.VMEM((heads, HEAD), f32),
        pltpu.VMEM((heads, HEAD), f32),
        pltpu.VMEM((n, batch, lane), bf16),
        pltpu.VMEM((n_tp, 8, lane), f32),
        pltpu.VMEM((n, 4, lane), f32),
        pltpu.VMEM((n, batch, lane), bf16),
        pltpu.VMEM((n, batch, lane), bf16),
        pltpu.VMEM((n, batch, lane), bf16),
        pltpu.VMEM((n_tp, n_kv, seqs, lane), f32),
        pltpu.VMEM((n, seqs, lane), f32),
        pltpu.VMEM((n_tp, batch, lane), bf16),
        pltpu.VMEM((n_kv, heads, HEAD), f32),
        pltpu.VMEM((n_kv, heads, HEAD), f32),
        pltpu.VMEM((n_kv, heads, HEAD), f32),
        pltpu.VMEM((4, batch * heads, HEAD), f32),
        pltpu.VMEM((4, n_kv, seq_rows, HEAD), bf16),
        pltpu.VMEM((4, n_kv, seq_rows, HEAD), bf16),
        pltpu.VMEM((seq_rows, HEAD), f32),
        pltpu.VMEM((parts, part_rows, lane), f32),
        pltpu.VMEM((parts, n_tp, part_rows, lane), bf16),
        pltpu.VMEM((parts, n_kv, part_rows, lane), bf16),
        pltpu.VMEM((parts, n_kv * part_rows, lane), f32),
        pltpu.VMEM((n_kv, 2 * seqs, lane), f32),
        pltpu.VMEM((n, batch, lane), bf16),
        pltpu.VMEM((n, 2, lane), f32),
        pltpu.VMEM((batch, lane), f32),
        pltpu.SemaphoreType.DMA((len(KINDS) + 4,)),
        pltpu.SemaphoreType.DMA((len(KINDS),)),
        pltpu.SemaphoreType.DMA((n_kv,)),
        pltpu.SemaphoreType.DMA((4,)),
        pltpu.SemaphoreType.DMA((parts,)),
        pltpu.SemaphoreType.DMA((parts,)),
        pltpu.SemaphoreType.DMA((17,)),
    ]
    vmem = pl.BlockSpec(memory_space=pltpu.VMEM)
    hbm = pl.BlockSpec(memory_space=pl.ANY)
    held = pl.pallas_call(
        functools.partial(layer_kernel, n_kv, n_tp),
        out_shape=(pltpu.VMEM(tokens.shape, bf16), pltpu.VMEM(state.shape, f32)),
        in_specs=[hbm] * 14,
        out_specs=(vmem, vmem),
        scratch_shapes=scratch,
        compiler_params=pltpu.CompilerParams(
            collective_id=0, has_side_effects=True, vmem_limit_bytes=58 * 1024 * 1024
        ),
        name="layer",
    )(*[pltpu.with_memory_space_constraint(operand, pltpu.HBM) for operand in (
        tokens,
        norm_gain,
        norm_bias,
        lower_bound.reshape(heads, HEAD),
        head_gain.reshape(heads, HEAD),
        gate_weights,
        up_weights,
        down_weights,
        query_weight,
        forget_weight,
        input_weight,
        outgate_weight,
        out_weight,
        state,
    )])
    return pl.pallas_call(
        store_kernel,
        out_shape=(
            jax.ShapeDtypeStruct(tokens.shape, bf16),
            jax.ShapeDtypeStruct(state.shape, f32),
        ),
        in_specs=[vmem, vmem],
        out_specs=(hbm, hbm),
        scratch_shapes=[pltpu.SemaphoreType.DMA((2,))],
        compiler_params=pltpu.CompilerParams(vmem_limit_bytes=4 * 1024 * 1024),
        name="store",
    )(*held)


def power_of_two(count):
    return count & (count - 1) == 0


def dispatch(n_kv, n_tp, *args):
    tokens, state = args[0], args[13]
    batch, lane = tokens.shape
    seqs, heads = state.shape[:2]
    fits = lane == HEAD and batch == 16 and heads == 8 and seqs == 2 and n_kv == 8
    if fits and power_of_two(n_tp) and n_kv * n_tp % 8 == 0:
        return fused(n_kv, n_tp, *args)
    return local(*args)


def solution(mesh):
    n_kv, n_tp = mesh.shape["kv"], mesh.shape["tp"]
    return jax.shard_map(
        functools.partial(dispatch, n_kv, n_tp),
        mesh=mesh,
        in_specs=(
            P(None, ("kv", "tp")),
            P(None, None, ("kv", "tp")),
            P(None, None, ("kv", "tp")),
            P(None, ("kv", "tp"), None),
            P(None, ("kv", "tp")),
            P(None, ("kv", "tp")),
            P("kv", "tp"),
            P("kv", "tp"),
            P("kv", "tp"),
            P("kv", "tp"),
            P("tp"),
            P("tp"),
            P("tp", None),
            P("kv", "tp", None, None),
        ),
        out_specs=(P(None, ("kv", "tp")), P("kv", "tp", None, None)),
        check_vma=False,
    )
```

```python
import functools

import jax
import jax.numpy as jnp
from jax import lax
from jax.experimental import pallas as pl
from jax.experimental.pallas import tpu as pltpu
from jax.sharding import PartitionSpec as P

MESH = pl.DeviceIdType.MESH

HEAD = 128


residual_scale = 8.0**0.25
norm_eps = 1e-05
head_eps = 1e-06


def whole_norm(stream, gain_row, bias_row):
    row_mean = jnp.mean(stream, axis=-1, keepdims=True)
    centred = stream - row_mean
    spread = jnp.mean(centred * centred, axis=-1, keepdims=True)
    return centred * lax.rsqrt(spread + norm_eps) * gain_row.astype(jnp.float32) + bias_row.astype(
        jnp.float32
    )


def ffn_partial(whole_rows, gate_w, up_w, down_w):
    gate_proj = jnp.dot(whole_rows, gate_w, preferred_element_type=jnp.float32)
    up_proj = jnp.dot(whole_rows, up_w, preferred_element_type=jnp.float32)
    hidden = (jax.nn.silu(gate_proj) * up_proj).astype(jnp.bfloat16)
    return jnp.dot(hidden, down_w, preferred_element_type=jnp.float32)


def local(
    tokens,
    gate_weights,
    up_weights,
    down_weights,
    norm_gain,
    norm_bias,
    query_weight,
    forget_weight,
    input_weight,
    outgate_weight,
    lower_bound,
    head_gain,
    out_weight,
    state,
):
    own_cols = tokens.shape[1]
    col_offset = lax.axis_index(("kv", "tp")) * own_cols
    whole_tokens, whole_gain, whole_bias = (
        lax.all_gather(tokens, ("kv", "tp"), axis=1, tiled=True),
        lax.all_gather(norm_gain, ("kv", "tp"), axis=1, tiled=True),
        lax.all_gather(norm_bias, ("kv", "tp"), axis=1, tiled=True),
    )

    def finish(partial_value, residual_whole, index, want_whole):
        total = lax.psum(partial_value, ("kv", "tp"))
        stream = residual_scale * residual_whole + 0.5 * total
        normed = whole_norm(stream, whole_gain[index], whole_bias[index]).astype(jnp.bfloat16)
        if want_whole:
            return normed
        return lax.dynamic_slice_in_dim(normed, col_offset, own_cols, 1)

    partial_one = ffn_partial(whole_tokens, gate_weights[0], up_weights[0], down_weights[0])
    normed_one = finish(partial_one, whole_tokens.astype(jnp.float32), 0, True)
    seq_count = state.shape[0]
    head_count = state.shape[1]
    head_cols = query_weight.shape[1]
    weight_rows = query_weight.shape[0]
    seq_offset = lax.axis_index("kv") * seq_count
    block_rows = lax.dynamic_slice_in_dim(
        normed_one, lax.axis_index("kv") * weight_rows, weight_rows, 1
    )
    weights = (query_weight, forget_weight, input_weight, outgate_weight)
    projected = lax.psum_scatter(
        jnp.concatenate(
            [jnp.dot(block_rows, weight, preferred_element_type=jnp.float32) for weight in weights],
            axis=1,
        ).astype(jnp.bfloat16),
        "kv",
        scatter_dimension=0,
        tiled=True,
    )
    query_pre = projected[:, :head_cols].astype(jnp.float32).reshape(seq_count, head_count, HEAD)
    forget_pre = (
        projected[:, head_cols : 2 * head_cols]
        .astype(jnp.float32)
        .reshape(seq_count, head_count, HEAD)
    )
    input_pre = (
        projected[:, 2 * head_cols : 3 * head_cols]
        .astype(jnp.float32)
        .reshape(seq_count, head_count, HEAD)
    )
    outgate_pre = projected[:, 3 * head_cols :].astype(jnp.float32)
    low_bound = lower_bound.reshape(head_count, HEAD)
    forget = low_bound + (1.0 - low_bound) * jax.nn.sigmoid(forget_pre)
    key_part = (1.0 - low_bound) * jax.nn.sigmoid(-forget_pre)
    updated = forget[..., None] * state + key_part[..., None] * input_pre[:, :, None, :]
    readout = jnp.einsum(
        "shd,shde->she", jax.nn.silu(query_pre), updated, precision=lax.Precision.HIGHEST
    )
    readout = readout * lax.rsqrt(jnp.mean(readout * readout, axis=-1, keepdims=True) + head_eps)
    gated_out = (
        readout.reshape(seq_count, head_cols) * head_gain * jax.nn.silu(outgate_pre)
    ).astype(jnp.bfloat16)
    mixer_part = jnp.dot(gated_out, out_weight, preferred_element_type=jnp.float32)
    head_sum = lax.psum_scatter(
        mixer_part.astype(jnp.bfloat16), "tp", scatter_dimension=1, tiled=True
    ).astype(jnp.float32)
    piece_cols = head_sum.shape[1]
    own_normed = lax.dynamic_slice_in_dim(normed_one, seq_offset, seq_count, 0)
    own_normed = lax.dynamic_slice_in_dim(
        own_normed, lax.axis_index("tp") * piece_cols, piece_cols, 1
    )
    stream_own = (residual_scale * own_normed.astype(jnp.float32) + head_sum).astype(jnp.bfloat16)
    seq_rows = lax.all_gather(stream_own, "tp", axis=1, tiled=True)
    stream_two = lax.all_gather(seq_rows, "kv", axis=0, tiled=True)
    normed_two = whole_norm(stream_two.astype(jnp.float32), whole_gain[1], whole_bias[1]).astype(
        jnp.bfloat16
    )
    partial_two = ffn_partial(normed_two, gate_weights[1], up_weights[1], down_weights[1])
    mixed = finish(partial_two, normed_two.astype(jnp.float32), 2, False)
    return (mixed, updated)


KINDS = ("gain_tp", "gains", "rs_one", "turn", "turn_tp", "own_tp", "base", "bases", "stat_two", "rs_three", "spread")


def tree_sum(terms):
    while len(terms) > 1:
        rest = [terms[-1]] if len(terms) % 2 else []
        terms = [a + b for a, b in zip(terms[::2], terms[1::2])] + rest
    return terms[0]


def total_of(tiles):
    rows = jnp.sum(tree_sum(tiles), axis=0, keepdims=True)
    return jnp.sum(rows, axis=1, keepdims=True)


def dot_turned(rows, weights):
    return lax.dot_general(
        rows, weights, (((1,), (1,)), ((), ())), preferred_element_type=jnp.float32
    )


def flipped(value, count, mask):
    out, bit = value, 1
    while bit < count:
        if mask & bit:
            out = out + bit - 2 * bit * lax.rem(lax.div(value, bit), 2)
        bit *= 2
    return out


def layer_kernel(
    n_kv,
    n_tp,
    tokens_hbm,
    gain_hbm,
    bias_hbm,
    low_hbm,
    head_gain_hbm,
    gate_hbm,
    up_hbm,
    down_hbm,
    query_hbm,
    forget_hbm,
    input_hbm,
    outgate_hbm,
    out_hbm,
    state_hbm,
    mixed_ref,
    new_v,
    gate_v,
    up_v,
    gate_t,
    up_t,
    down_v,
    proj_v,
    out_v,
    state_v,
    gain_v,
    bias_v,
    low_v,
    head_gain_v,
    tok_buf,
    gain_tp,
    gain_buf,
    rs_send,
    rs_recv_one,
    rs_recv_three,
    turn_tp,
    turn_recv,
    own_tp,
    base_send,
    base_recv,
    base_all,
    proj_f32,
    proj_send,
    proj_recv,
    gated_buf,
    head_f32,
    head_buf,
    ag_two,
    ag_two_f32,
    stat_two,
    normed_bf,
    spread_buf,
    final_buf,
    send_sem,
    recv_sem,
    tok_sem,
    proj_sem,
    head_sem,
    ag_sem,
    load_sem,
):
    n = n_kv * n_tp
    batch, lane = tok_buf.shape[1:]
    width = n * lane
    seqs, heads = state_v.shape[0], state_v.shape[1]
    part_rows = ag_two.shape[2]
    per = part_rows // seqs
    parts = n // per
    group = n_tp * lane
    bf16, f32 = jnp.bfloat16, jnp.float32
    kv, tp = lax.axis_index("kv"), lax.axis_index("tp")
    me = kv * n_tp + tp
    kv_of = [flipped(kv, n_kv, m) for m in range(n_kv)]
    tp_of = [flipped(tp, n_tp, m) for m in range(n_tp)]
    peers = [(k, t) for k in reversed(range(n_kv)) for t in reversed(range(n_tp)) if k or t]

    barrier = pltpu.get_barrier_semaphore()
    for k, t in peers:
        pl.semaphore_signal(
            barrier, inc=1, device_id=(kv_of[k], tp_of[t]), device_id_type=MESH
        )

    proj_hbm = (query_hbm, forget_hbm, input_hbm, outgate_hbm)
    loads = {}
    order = [("tokens", tokens_hbm, tok_buf.at[me])]
    order += [("gain", gain_hbm, gain_v), ("bias", bias_hbm, bias_v)]
    order += [("gate0", gate_hbm.at[0], gate_v.at[0]), ("up0", up_hbm.at[0], up_v.at[0])]
    order += [("down0", down_hbm.at[0], down_v.at[0])]
    order += [("proj%d" % i, proj_hbm[i], proj_v.at[i]) for i in range(4)]
    order += [("low", low_hbm, low_v), ("head_gain", head_gain_hbm, head_gain_v)]
    order += [("state", state_hbm, state_v), ("out", out_hbm, out_v)]
    order += [("gate1", gate_hbm.at[1], gate_v.at[1]), ("up1", up_hbm.at[1], up_v.at[1])]
    order += [("down1", down_hbm.at[1], down_v.at[1])]
    for i, (name, source, target) in enumerate(order):
        loads[name] = pltpu.make_async_copy(source, target, load_sem.at[i])
        if i < 10:
            loads[name].start()

    def send(src, dst, kind, recv, k, t):
        pltpu.make_async_remote_copy(
            src_ref=src,
            dst_ref=dst,
            send_sem=send_sem.at[kind],
            recv_sem=recv,
            device_id=(kv_of[k], tp_of[t]),
            device_id_type=MESH,
        ).start()

    def wait_for(sem, ref, count):
        part = ref.at[pl.ds(0, count)]
        pltpu.make_async_copy(part, part, sem).wait()

    GAIN_TP, GAINS, RS_ONE, TURN, TURN_TP, OWN_TP, BASE, BASES, STAT_TWO, RS_THREE, SPREAD = range(len(KINDS))
    TOK, PROJ, HEADS_SUM, AG_TWO = range(len(KINDS), len(KINDS) + 4)

    loads["gain"].wait()
    loads["bias"].wait()
    pad = jnp.zeros((2, lane), f32)
    gains, biases = gain_v[...].astype(f32), bias_v[...].astype(f32)
    gains = jnp.concatenate([gains[0:2], biases[0:2], gains[2:3], biases[2:3], pad], axis=0)
    gain_tp[tp] = gains
    loads["tokens"].wait()
    pl.semaphore_wait(barrier, n - 1)
    for k, t in peers:
        send(tok_buf.at[me], tok_buf.at[me], TOK, tok_sem.at[kv], k, t)
    for t in reversed(range(1, n_tp)):
        send(gain_tp.at[tp], gain_tp.at[tp], GAIN_TP, recv_sem.at[GAIN_TP], 0, t)

    for name in [entry[0] for entry in order[10:]]:
        loads[name].start()

    def columns(index, size):
        return pl.ds(pl.multiple_of(index * size, size), size)

    def hidden_of(gate, up):
        return (jax.nn.silu(gate) * up).astype(bf16)

    def reduce_scatter_start(hidden, layer, kind, recv):
        loads["down%d" % layer].wait()
        for k in reversed(range(n_kv)):
            target = kv_of[k]
            part = jnp.dot(
                hidden, down_v[layer, :, columns(target, group)], preferred_element_type=f32
            ).astype(bf16)
            for t in range(n_tp):
                rs_send[target * n_tp + t] = part[:, t * lane : (t + 1) * lane]
            for t in reversed(range(n_tp)):
                if k or t:
                    index = target * n_tp + tp_of[t]
                    send(rs_send.at[index], recv.at[me], kind, recv_sem.at[kind], k, t)
        recv[me] = rs_send[me]

    def reduce_scatter_end(kind, recv):
        wait_for(recv_sem.at[kind], recv, n - 1)
        return tree_sum([recv[j].astype(f32) for j in range(n)])

    def turn_weights(layer):
        loads["gate%d" % layer].wait()
        loads["up%d" % layer].wait()
        for source, target in ((gate_v, gate_t), (up_v, up_t)):

            @pl.loop(0, width // (2 * lane))
            def _(i):
                rows = columns(i, 2 * lane)
                target[layer, rows, :] = source[layer, :, rows].T

    def send_bases():
        wait_for(recv_sem.at[GAIN_TP], gain_tp, n_tp - 1)
        for t in range(n_tp):
            gain_buf[kv * n_tp + t] = gain_tp[t, 0:4]
        own_gains = gain_tp.at[:, pl.ds(0, 4)]
        for k in reversed(range(1, n_kv)):
            target = gain_buf.at[pl.ds(kv * n_tp, n_tp)]
            send(own_gains, target, GAINS, recv_sem.at[GAINS], k, 0)
        kv_gains = jnp.concatenate([gain_tp[t] for t in range(n_tp)], axis=1).astype(bf16)
        for i in range(4):
            loads["proj%d" % i].wait()
            based = jnp.dot(kv_gains, proj_v[i], preferred_element_type=f32)
            for h in range(heads):
                block = slice(h * HEAD, (h + 1) * HEAD)
                base_send[2 * i, h : h + 1, :] = based[0:1, block]
                base_send[2 * i + 1, h : h + 1, :] = based[2:3, block]
        for k in reversed(range(1, n_kv)):
            send(base_send.at[kv_of[k]], base_recv.at[kv], BASE, recv_sem.at[BASE], k, 0)
        base_recv[kv] = base_send[kv]

    turn_weights(0)
    gate = up = None
    for k in range(0, n_kv, 2):
        sources = (kv_of[k], kv_of[k + 1])
        for i, source in enumerate(sources):
            wait_for(tok_sem.at[source], tok_buf, n_tp if k + i else n_tp - 1)
        low_group = lax.div(kv_of[k], 2)
        rows = jnp.concatenate(
            [tok_buf[low_group * 2 * n_tp + t] for t in range(2 * n_tp)], axis=1
        )
        cols = columns(low_group, 2 * group)
        gate_part = jnp.dot(rows, gate_t[0, cols, :], preferred_element_type=f32)
        up_part = jnp.dot(rows, up_t[0, cols, :], preferred_element_type=f32)
        gate = gate_part if gate is None else gate + gate_part
        up = up_part if up is None else up + up_part
    reduce_scatter_start(hidden_of(gate, up), 0, RS_ONE, rs_recv_one)

    send_bases()
    turn_weights(1)
    token_sum = jnp.sum(
        tree_sum([tok_buf[j].astype(f32) for j in range(n)]), axis=1, keepdims=True
    )
    centre = residual_scale * token_sum / width
    own_tokens = residual_scale * tok_buf[me].astype(f32) - centre

    shifted = own_tokens + 0.5 * reduce_scatter_end(RS_ONE, rs_recv_one)
    own_tp[tp] = (shifted * gains[0:1, :]).astype(bf16)
    for t in reversed(range(1, n_tp)):
        send(own_tp.at[tp], own_tp.at[tp], OWN_TP, recv_sem.at[OWN_TP], 0, t)
    for j in range(n_kv):
        turn_tp[tp, j] = shifted[j * seqs : (j + 1) * seqs, :]
    for t in reversed(range(1, n_tp)):
        send(turn_tp.at[tp], turn_tp.at[tp], TURN_TP, recv_sem.at[TURN_TP], 0, t)

    wait_for(recv_sem.at[BASE], base_recv, n_kv - 1)
    base_all[kv] = tree_sum([base_recv[j] for j in range(n_kv)])
    for k in reversed(range(1, n_kv)):
        send(base_all.at[kv], base_all.at[kv], BASES, recv_sem.at[BASES], k, 0)
    wait_for(recv_sem.at[OWN_TP], own_tp, n_tp - 1)
    block = jnp.concatenate([own_tp[t] for t in range(n_tp)], axis=1)
    wait_for(recv_sem.at[TURN_TP], turn_tp, n_tp - 1)
    own_turn = turn_recv.at[pl.ds(kv * n_tp, n_tp)]
    for k in reversed(range(1, n_kv)):
        send(turn_tp.at[:, kv_of[k]], own_turn, TURN, recv_sem.at[TURN], k, 0)
    for t in range(n_tp):
        turn_recv[kv * n_tp + t] = turn_tp[t, kv]
    turns = (1, 2, 0, 3)
    for i in turns:
        part = jnp.dot(block, proj_v[i], preferred_element_type=f32)
        for h in range(heads):
            for r in range(0, batch, 8):
                proj_f32[i, pl.ds(r * heads + h, 8, stride=heads), :] = part[
                    r : r + 8, h * HEAD : (h + 1) * HEAD
                ]
        proj_send[i] = proj_f32[i].reshape(proj_send.shape[1:]).astype(bf16)
        for k in reversed(range(1, n_kv)):
            send(proj_send.at[i, kv_of[k]], proj_recv.at[i, kv], PROJ, proj_sem.at[i], k, 0)
        proj_recv[i, kv] = proj_send[i, kv]

    wait_for(recv_sem.at[GAINS], gain_buf, n - n_tp)
    all_gains = jnp.concatenate([gain_buf[j] for j in range(n)], axis=1).astype(bf16)
    gate_fixed = jnp.dot(all_gains, gate_t[1], preferred_element_type=f32)
    up_fixed = jnp.dot(all_gains, up_t[1], preferred_element_type=f32)
    wait_for(recv_sem.at[TURN], turn_recv, n - n_tp)

    def norm_stats(tiles):
        mean = total_of(tiles) / width
        centred = [tile - mean for tile in tiles]
        scale = lax.rsqrt(total_of([c * c for c in centred]) / width + norm_eps)
        return mean, scale, centred

    def normed_rows(stats, index):
        return [
            (
                tile * stats[1] * gain_buf[c * per : (c + 1) * per, index, :]
                + gain_buf[c * per : (c + 1) * per, 2 + index, :]
            ).astype(bf16)
            for c, tile in enumerate(stats[2])
        ]

    norm_one = [
        norm_stats([turn_recv[c * per : (c + 1) * per, s, :] for c in range(parts)])
        for s in range(seqs)
    ]
    wait_for(recv_sem.at[BASES], base_all, n_kv - 1)

    def projected(i):
        wait_for(proj_sem.at[i], proj_recv.at[i], n_kv - 1)
        total = tree_sum([proj_recv[i, j].astype(f32) for j in range(n_kv)])
        found = []
        for s in range(seqs):
            mean, scale, _ = norm_one[s]
            rows = total[s * heads : (s + 1) * heads] - mean * base_all[2 * i]
            rows = scale * rows + base_all[2 * i + 1]
            found.append(rows.astype(bf16).astype(f32))
        return found

    loads["low"].wait()
    low = low_v[...]
    forget_pre = projected(1)
    forget = [low + (1.0 - low) * jax.nn.sigmoid(p) for p in forget_pre]
    key_part = [(1.0 - low) * jax.nn.sigmoid(-p) for p in forget_pre]
    input_pre = projected(2)
    query = [jax.nn.silu(p) for p in projected(0)]
    fill = jnp.zeros((HEAD - 3 * seqs * heads, HEAD), f32)
    seen = [q * f for q, f in zip(query, forget)]
    turned = jnp.concatenate([*seen, *forget, *key_part, fill], axis=0).T

    def column(kind, s, h):
        first = (kind * seqs + s) * heads + h
        return turned[:, first : first + 1]

    loads["state"].wait()
    readouts = []
    for s in range(seqs):
        rows = [
            jnp.sum(column(0, s, h) * state_v[s, h], axis=0, keepdims=True) for h in range(heads)
        ]
        match = jnp.sum(query[s] * key_part[s], axis=1, keepdims=True)
        readout = jnp.concatenate(rows, axis=0) + match * input_pre[s]
        mean_square = jnp.mean(readout * readout, axis=1, keepdims=True)
        readouts.append(readout * lax.rsqrt(mean_square + head_eps))
    loads["head_gain"].wait()
    outgate = projected(3)
    for s in range(seqs):
        gated_buf[s * heads : (s + 1) * heads, :] = (
            readouts[s] * head_gain_v[...] * jax.nn.silu(outgate[s])
        )
    gated = jnp.concatenate(
        [gated_buf[pl.ds(h, seqs, stride=heads), :] for h in range(heads)], axis=1
    ).astype(bf16)
    loads["out"].wait()
    step = per * lane
    for c in range(parts):
        part = jnp.dot(gated, out_v[:, c * step : (c + 1) * step], preferred_element_type=f32)
        for j in range(per):
            head_f32[c, pl.ds(j, seqs, stride=per), :] = part[:, j * lane : (j + 1) * lane]
        head_buf[c, tp] = head_f32[c].astype(bf16)
        for t in reversed(range(1, n_tp)):
            send(head_buf.at[c, tp], head_buf.at[c, tp], HEADS_SUM, head_sem.at[c], 0, t)

    for s in range(seqs):
        for h in range(heads):
            new_v[s, h] = (
                column(1, s, h) * state_v[s, h] + column(2, s, h) * input_pre[s][h : h + 1, :]
            )

    residual = [
        [residual_scale * tile.astype(f32) for tile in normed_rows(norm_one[s], 0)]
        for s in range(seqs)
    ]
    middle = [total_of(residual[s]) / width for s in range(seqs)]
    streams = [[] for _ in range(seqs)]
    for c in range(parts):
        wait_for(head_sem.at[c], head_buf.at[c], n_tp - 1)
        head_total = tree_sum([head_buf[c, t].astype(f32) for t in range(n_tp)])
        for s in range(seqs):
            mixed_rows = residual[s][c] + head_total[s * per : (s + 1) * per]
            streams[s].append(mixed_rows.astype(bf16).astype(f32) - middle[s])
        gain_rows = gain_buf[c * per : (c + 1) * per, 1, :]
        ag_two[c, kv] = jnp.concatenate(
            [streams[s][c] * gain_rows for s in range(seqs)], axis=0
        ).astype(bf16)
        for k in reversed(range(1, n_kv)):
            send(ag_two.at[c, kv], ag_two.at[c, kv], AG_TWO, ag_sem.at[c], k, 0)
    stats = [norm_stats(streams[s]) for s in range(seqs)]
    for i in range(2):
        for s in range(seqs):
            row = jnp.broadcast_to(stats[s][i], (1, lane))
            stat_two[kv, i * seqs + s : i * seqs + s + 1, :] = row
    for k in reversed(range(1, n_kv)):
        send(stat_two.at[kv], stat_two.at[kv], STAT_TWO, recv_sem.at[STAT_TWO], k, 0)

    wait_for(send_sem.at[RS_ONE], rs_recv_one, n - 1)
    gate = up = None
    for c in range(parts):
        wait_for(ag_sem.at[c], ag_two.at[c], n_kv - 1)
        ag_two_f32[c] = ag_two[c].astype(f32).reshape(ag_two_f32.shape[1:])
        tiles = []
        for j in range(per):
            pieces = [
                ag_two_f32[c, pl.ds(s * per + j, n_kv, stride=part_rows), :] for s in range(seqs)
            ]
            tiles.append(jnp.concatenate(pieces, axis=0).astype(bf16))
            normed_bf[c * per + j] = tiles[-1]
        rows = jnp.concatenate(tiles, axis=1)
        cols = slice(c * step, (c + 1) * step)
        gate_part = jnp.dot(rows, gate_t[1, cols, :], preferred_element_type=f32)
        up_part = jnp.dot(rows, up_t[1, cols, :], preferred_element_type=f32)
        gate = gate_part if gate is None else gate + gate_part
        up = up_part if up is None else up + up_part
    wait_for(recv_sem.at[STAT_TWO], stat_two, n_kv - 1)
    mean_two, scale_two = [
        jnp.concatenate([stat_two[:, i * seqs + s, :] for s in range(seqs)], axis=0)[:, 0:1]
        for i in range(2)
    ]
    gate = scale_two * (gate - mean_two * gate_fixed[1:2]) + gate_fixed[3:4]
    up = scale_two * (up - mean_two * up_fixed[1:2]) + up_fixed[3:4]
    reduce_scatter_start(hidden_of(gate, up), 1, RS_THREE, rs_recv_three)
    own_rows = scale_two * (normed_bf[me].astype(f32) - mean_two * gains[1:2]) + gains[3:4]
    own_rows = residual_scale * own_rows

    row_ids = lax.broadcasted_iota(jnp.int32, (batch, lane), 0)
    lane_ids = lax.broadcasted_iota(jnp.int32, (batch, lane), 1)
    stream = own_rows + 0.5 * reduce_scatter_end(RS_THREE, rs_recv_three)
    own_mean = jnp.sum(stream, axis=1, keepdims=True) / lane
    own_centred = stream - own_mean
    own_spread = jnp.sum(own_centred * own_centred, axis=1, keepdims=True)

    def to_lanes(values):
        return jnp.sum(jnp.where(row_ids == lane_ids, values, 0.0), axis=0, keepdims=True)

    spread_buf[me] = jnp.concatenate([to_lanes(own_mean), to_lanes(own_spread)], axis=0)
    for k, t in peers:
        send(spread_buf.at[me], spread_buf.at[me], SPREAD, recv_sem.at[SPREAD], k, t)

    for s in range(seqs):
        final_buf[pl.ds(s, n_kv, stride=seqs), :] = stream[s * n_kv : (s + 1) * n_kv, :]
    natural = final_buf[...]
    for kind in (TOK, RS_THREE):
        wait_for(send_sem.at[kind], tok_buf, n - 1)
    wait_for(send_sem.at[GAINS], gain_buf, n - n_tp)
    wait_for(send_sem.at[TURN_TP], turn_tp, n_tp - 1)
    wait_for(send_sem.at[GAIN_TP], gain_tp, n_tp - 1)
    wait_for(send_sem.at[TURN], turn_recv, n - n_tp)
    wait_for(send_sem.at[OWN_TP], own_tp, n_tp - 1)
    wait_for(send_sem.at[BASE], base_recv, n_kv - 1)
    wait_for(send_sem.at[BASES], base_all, n_kv - 1)
    for i in range(4):
        wait_for(send_sem.at[PROJ], proj_recv.at[i], n_kv - 1)
    wait_for(send_sem.at[STAT_TWO], stat_two, n_kv - 1)
    for c in range(parts):
        wait_for(send_sem.at[HEADS_SUM], head_buf.at[c], n_tp - 1)
        wait_for(send_sem.at[AG_TWO], ag_two.at[c], n_kv - 1)

    wait_for(recv_sem.at[SPREAD], spread_buf, n - 1)
    means = spread_buf[:, 0, :]
    mean_row = jnp.sum(means, axis=0, keepdims=True) / n
    apart = means - mean_row
    square_row = jnp.sum(spread_buf[:, 1, :] + lane * (apart * apart), axis=0, keepdims=True)
    scale_row = lax.rsqrt(square_row / width + norm_eps)
    place = lax.rem(row_ids, seqs) * n_kv + lax.div(row_ids, seqs)

    def to_rows(values):
        return jnp.sum(jnp.where(place == lane_ids, values, 0.0), axis=1, keepdims=True)

    mixed = (natural - to_rows(mean_row)) * to_rows(scale_row) * gains[4:5, :] + gains[5:6, :]
    mixed_ref[...] = mixed.astype(bf16)
    wait_for(send_sem.at[SPREAD], spread_buf, n - 1)


def store_kernel(mixed_v, new_v, mixed_out, state_out, sem):
    copies = [
        pltpu.make_async_copy(new_v, state_out, sem.at[0]),
        pltpu.make_async_copy(mixed_v, mixed_out, sem.at[1]),
    ]
    for copy in copies:
        copy.start()
    for copy in copies:
        copy.wait()


def fused(n_kv, n_tp, *args):
    (
        tokens,
        gate_weights,
        up_weights,
        down_weights,
        norm_gain,
        norm_bias,
        query_weight,
        forget_weight,
        input_weight,
        outgate_weight,
        lower_bound,
        head_gain,
        out_weight,
        state,
    ) = args
    batch, lane = tokens.shape
    n = n_kv * n_tp
    seqs, heads = state.shape[:2]
    gate_weights = jnp.swapaxes(gate_weights, 1, 2)
    up_weights = jnp.swapaxes(up_weights, 1, 2)
    bf16, f32 = jnp.bfloat16, jnp.float32
    per = 8
    parts, part_rows = n // per, per * seqs
    seq_rows = seqs * heads
    scratch = [
        pltpu.VMEM(gate_weights.shape, bf16),
        pltpu.VMEM(up_weights.shape, bf16),
        pltpu.VMEM((2, n * lane, gate_weights.shape[1]), bf16),
        pltpu.VMEM((2, n * lane, gate_weights.shape[1]), bf16),
        pltpu.VMEM(down_weights.shape, bf16),
        pltpu.VMEM((4, *query_weight.shape), bf16),
        pltpu.VMEM(out_weight.shape, bf16),
        pltpu.VMEM(state.shape, f32),
        pltpu.VMEM(norm_gain.shape, bf16),
        pltpu.VMEM(norm_bias.shape, bf16),
        pltpu.VMEM((heads, HEAD), f32),
        pltpu.VMEM((heads, HEAD), f32),
        pltpu.VMEM((n, batch, lane), bf16),
        pltpu.VMEM((n_tp, 8, lane), f32),
        pltpu.VMEM((n, 4, lane), f32),
        pltpu.VMEM((n, batch, lane), bf16),
        pltpu.VMEM((n, batch, lane), bf16),
        pltpu.VMEM((n, batch, lane), bf16),
        pltpu.VMEM((n_tp, n_kv, seqs, lane), f32),
        pltpu.VMEM((n, seqs, lane), f32),
        pltpu.VMEM((n_tp, batch, lane), bf16),
        pltpu.VMEM((n_kv, heads, HEAD), f32),
        pltpu.VMEM((n_kv, heads, HEAD), f32),
        pltpu.VMEM((n_kv, heads, HEAD), f32),
        pltpu.VMEM((4, batch * heads, HEAD), f32),
        pltpu.VMEM((4, n_kv, seq_rows, HEAD), bf16),
        pltpu.VMEM((4, n_kv, seq_rows, HEAD), bf16),
        pltpu.VMEM((seq_rows, HEAD), f32),
        pltpu.VMEM((parts, part_rows, lane), f32),
        pltpu.VMEM((parts, n_tp, part_rows, lane), bf16),
        pltpu.VMEM((parts, n_kv, part_rows, lane), bf16),
        pltpu.VMEM((parts, n_kv * part_rows, lane), f32),
        pltpu.VMEM((n_kv, 2 * seqs, lane), f32),
        pltpu.VMEM((n, batch, lane), bf16),
        pltpu.VMEM((n, 2, lane), f32),
        pltpu.VMEM((batch, lane), f32),
        pltpu.SemaphoreType.DMA((len(KINDS) + 4,)),
        pltpu.SemaphoreType.DMA((len(KINDS),)),
        pltpu.SemaphoreType.DMA((n_kv,)),
        pltpu.SemaphoreType.DMA((4,)),
        pltpu.SemaphoreType.DMA((parts,)),
        pltpu.SemaphoreType.DMA((parts,)),
        pltpu.SemaphoreType.DMA((17,)),
    ]
    vmem = pl.BlockSpec(memory_space=pltpu.VMEM)
    hbm = pl.BlockSpec(memory_space=pl.ANY)
    held = pl.pallas_call(
        functools.partial(layer_kernel, n_kv, n_tp),
        out_shape=(pltpu.VMEM(tokens.shape, bf16), pltpu.VMEM(state.shape, f32)),
        in_specs=[hbm] * 14,
        out_specs=(vmem, vmem),
        scratch_shapes=scratch,
        compiler_params=pltpu.CompilerParams(
            collective_id=0, has_side_effects=True, vmem_limit_bytes=58 * 1024 * 1024
        ),
        name="layer",
    )(*[pltpu.with_memory_space_constraint(operand, pltpu.HBM) for operand in (
        tokens,
        norm_gain,
        norm_bias,
        lower_bound.reshape(heads, HEAD),
        head_gain.reshape(heads, HEAD),
        gate_weights,
        up_weights,
        down_weights,
        query_weight,
        forget_weight,
        input_weight,
        outgate_weight,
        out_weight,
        state,
    )])
    return pl.pallas_call(
        store_kernel,
        out_shape=(
            jax.ShapeDtypeStruct(tokens.shape, bf16),
            jax.ShapeDtypeStruct(state.shape, f32),
        ),
        in_specs=[vmem, vmem],
        out_specs=(hbm, hbm),
        scratch_shapes=[pltpu.SemaphoreType.DMA((2,))],
        compiler_params=pltpu.CompilerParams(vmem_limit_bytes=4 * 1024 * 1024),
        name="store",
    )(*held)


def power_of_two(count):
    return count & (count - 1) == 0


def dispatch(n_kv, n_tp, *args):
    tokens, state = args[0], args[13]
    batch, lane = tokens.shape
    seqs, heads = state.shape[:2]
    fits = lane == HEAD and batch == 16 and heads == 8 and seqs == 2 and n_kv == 8
    if fits and power_of_two(n_tp) and n_kv * n_tp % 8 == 0:
        return fused(n_kv, n_tp, *args)
    return local(*args)


def solution(mesh):
    n_kv, n_tp = mesh.shape["kv"], mesh.shape["tp"]
    return jax.shard_map(
        functools.partial(dispatch, n_kv, n_tp),
        mesh=mesh,
        in_specs=(
            P(None, ("kv", "tp")),
            P(None, None, ("kv", "tp")),
            P(None, None, ("kv", "tp")),
            P(None, ("kv", "tp"), None),
            P(None, ("kv", "tp")),
            P(None, ("kv", "tp")),
            P("kv", "tp"),
            P("kv", "tp"),
            P("kv", "tp"),
            P("kv", "tp"),
            P("tp"),
            P("tp"),
            P("tp", None),
            P("kv", "tp", None, None),
        ),
        out_specs=(P(None, ("kv", "tp")), P("kv", "tp", None, None)),
        check_vma=False,
    )
```
